128 devices in a mesh: fs: 16 (over z, x), tp: 8 (over y, core).
Axes of the slice: x: 4, y: 4, z: 4, core: 2. Of those that a mesh axis runs over, the one named last changes fastest.
Arguments:
- saved_input: bfloat16 [49152, 2048], P('fs'), may hold values from -24 to 24
- key_cot: bfloat16 [49152, 2048], P('fs', 'tp')
- value_cot: bfloat16 [49152, 2048], P('fs', 'tp')
- weights: float32 [2, 2048, 2048], P(None, 'fs', 'tp'), may hold values from -3 to 3
- left_root: float32 [2, 8, 2048, 2048], P(None, 'tp', 'fs'), may hold values from -1 to 3
- left_stat: float32 [2, 8, 2048, 2048], P(None, 'tp', 'fs'), may hold values from -48 to 48
- right_root: float32 [2, 8, 256, 256], P(None, 'tp'), may hold values from -1 to 3
- right_stat: float32 [2, 8, 256, 256], P(None, 'tp'), may hold values from -48 to 48
Outputs:
- step: float32 [2, 2048, 2048], P(None, 'fs', 'tp')
- new_weights: float32 [2, 2048, 2048], P(None, 'fs', 'tp')
- copies: bfloat16 [2, 2048, 2048], P(None, None, 'tp')
- new_left: float32 [2, 8, 2048, 2048], P(None, 'tp', 'fs')
- new_right: float32 [2, 8, 256, 256], P(None, 'tp')
The draws below stay inside these ranges and needn't reach their ends.
All inputs are finite; a program needn't handle non-finite values.
Results may differ from the reference program's by a relative error of at most 0.0004.
Values may be sent and summed in bfloat16 or wider, within the bound.
No kernel may reach another device: no remote copies, remote signals or barrier semaphores. Data moves between devices by JAX's collectives and lax.ppermute only.
A program may use at most 128 MiB of HBM per device.

```python
import jax
import jax.numpy as jnp
from jax import lax

D = 2048
KEY = 2048
BLK = 256
TOKENS = 49152
NBLK = 8


def rising(count, low, high):
    steps = jnp.arange(count, dtype=jnp.float32) / max(count - 1, 1)
    return low * (high / low) ** steps


def rough_noise(key, shape):
    return jnp.clip(jax.random.normal(jax.random.fold_in(key, 5), shape, jnp.float32), -6.0, 6.0)


def dominant(key, shape):
    width = shape[-1]
    diag = jax.random.uniform(jax.random.fold_in(key, 1), shape[:-1], jnp.float32, 0.5, 2.0)
    off = jax.random.normal(jax.random.fold_in(key, 2), shape, jnp.float32)
    off = jnp.clip(off, -6.0, 6.0) * (0.4 / width ** 0.5)
    return off + diag[..., None] * jnp.eye(width, dtype=jnp.float32)


def draw_saved_input(key, part):
    values = rough_noise(jax.random.fold_in(key, 11), (TOKENS, D))
    values = values * rising(D, 0.3, 3.0)[None, :] * rising(TOKENS, 0.6, 1.3)[:, None]
    return jnp.clip(values, -24.0, 24.0).astype(jnp.bfloat16)


def draw_key_cot(key, part):
    values = rough_noise(jax.random.fold_in(key, 12), (TOKENS, KEY))
    values = values * rising(KEY, 0.3, 3.0)[None, :] * TOKENS ** (-0.5)
    return values.astype(jnp.bfloat16)


def draw_value_cot(key, part):
    values = rough_noise(jax.random.fold_in(key, 13), (TOKENS, KEY))
    values = values * rising(KEY, 3.0, 0.3)[None, :] * TOKENS ** (-0.5)
    return values.astype(jnp.bfloat16)


def draw_left_root(key, part):
    return dominant(jax.random.fold_in(key, 14), (2, NBLK, D, D))


def draw_right_root(key, part):
    return dominant(jax.random.fold_in(key, 15), (2, NBLK, BLK, BLK))


def steps_of(key, extent, pieces, least, largest):
    def one(dim, blocks):
        steps = jax.random.uniform(jax.random.fold_in(jax.random.fold_in(key, 6), dim), (blocks,), jnp.float32, least / len(pieces), largest / len(pieces))
        return jnp.repeat(jnp.exp(steps), extent[dim] // blocks).reshape((-1,) + (1,) * (len(extent) - dim - 1))

    loudness = one(*pieces[0])
    for cut in pieces[1:]:
        loudness = loudness * one(*cut)
    return loudness


def normal_values(own_key, shape, scale, limit, shards=(), held_as=jnp.bfloat16):
    drawn = scale * jax.random.normal(own_key, shape, jnp.float32)
    if shards:
        drawn = drawn * steps_of(own_key, shape, shards, -0.22, 0.18)
    return jnp.clip(drawn, -limit, limit).astype(held_as)


def setup_inputs(seed: int = 0) -> dict:
    key_of = jax.random.split(jax.random.key(seed), 9)
    return {
        "saved_input": draw_saved_input(jax.random.fold_in(key_of[8], 71), 0),
        "key_cot": draw_key_cot(jax.random.fold_in(key_of[8], 71), 0),
        "value_cot": draw_value_cot(jax.random.fold_in(key_of[8], 71), 0),
        "weights": normal_values(key_of[3], (2, D, KEY), 0.2, 3.0, ((1, 16), (2, 8)), jnp.float32),
        "left_root": draw_left_root(jax.random.fold_in(key_of[8], 71), 0),
        "left_stat": normal_values(key_of[5], (2, NBLK, D, D), 8.0, 48.0, ((1, 8), (2, 16)), jnp.float32),
        "right_root": draw_right_root(jax.random.fold_in(key_of[8], 71), 0),
        "right_stat": normal_values(key_of[7], (2, NBLK, BLK, BLK), 8.0, 48.0, ((1, 8),), jnp.float32),
    }


decay_stat = 0.9
learn_rate = 0.05
norm_eps = 1e-06

def reference(saved_input, key_cot, value_cot, weights, left_root, left_stat, right_root, right_stat):
    hi = lax.Precision.HIGHEST
    grads = jnp.stack([jnp.dot(saved_input.T, key_cot, preferred_element_type=jnp.float32), jnp.dot(saved_input.T, value_cot, preferred_element_type=jnp.float32)])
    blocks = grads.reshape(2, D, NBLK, BLK).transpose(0, 2, 1, 3)
    pre = jnp.einsum('mbrk,mbkc->mbrc', left_root, blocks, precision=hi)
    raw = jnp.einsum('mbrc,mbcd->mbrd', pre, right_root, precision=hi)
    new_left = decay_stat * left_stat + (1.0 - decay_stat) * jnp.einsum('mbrc,mbkc->mbrk', blocks, blocks, precision=hi)
    new_right = decay_stat * right_stat + (1.0 - decay_stat) * jnp.einsum('mbrc,mbrd->mbcd', blocks, blocks, precision=hi)
    grad_sq = lax.optimization_barrier(jnp.sum(grads * grads, axis=(1, 2)))
    raw_sq = lax.optimization_barrier(jnp.sum(raw * raw, axis=(1, 2, 3)))
    scale = jnp.sqrt(grad_sq / (raw_sq + norm_eps))
    step = (scale[:, None, None, None] * raw).transpose(0, 2, 1, 3).reshape(2, D, KEY)
    new_weights = weights - learn_rate * step
    copies = new_weights.astype(jnp.bfloat16)
    return (step, new_weights, copies, new_left, new_right)
```

```python
import functools

import jax
import jax.numpy as jnp
from jax import lax
from jax.experimental import pallas as pl
from jax.experimental.pallas import tpu as pltpu
from jax.sharding import Mesh
from jax.sharding import PartitionSpec as P

FS = ("fs_0", "fs_1")
FS_TP = ("fs_0", "fs_1", "tp_0", "tp_1")
TP = ("tp_0", "tp_1")
Z, X = FS
RING = 4

decay_stat = 0.9
learn_rate = 0.05
norm_eps = 1e-06


VMEM = pl.BlockSpec(memory_space=pltpu.VMEM)
SMEM = pl.BlockSpec(memory_space=pltpu.SMEM)


def shift(value, axis, by):
    return lax.ppermute(value, axis, [(i, (i + by) % RING) for i in range(RING)])


def at(blocks, index):
    return lax.dynamic_index_in_dim(blocks, index % RING, 0, keepdims=False)


def split(value):
    high = value.astype(jnp.bfloat16)
    return high, (value - high.astype(jnp.float32)).astype(jnp.bfloat16)


def dot3(left, right, dims):
    (lh, ll), (rh, rl) = left, right
    dot = functools.partial(
        lax.dot_general, dimension_numbers=(dims, ((), ())), preferred_element_type=jnp.float32
    )
    return dot(lh, rh) + (dot(lh, rl) + dot(ll, rh))


def partial_kernel(count, width, xs, zs, *refs):
    cots = refs[:2]
    tiles = refs[2 : 2 + count * 5]
    outs = refs[2 + count * 5 :]
    first = pl.program_id(0) == 0
    turned = [c[...].T for c in cots]
    for i in range(count):
        own = tiles[i * 5 : i * 5 + 5]
        by_x = jnp.concatenate([t[...] for t in own[:4]], axis=1)
        for out, lhs, rhs in ((outs[2 * i], turned[0], by_x), (outs[2 * i + 1], turned[1], own[4][...])):
            total = jnp.dot(lhs, rhs, preferred_element_type=jnp.float32)

            @pl.when(first)
            def _():
                for j in range(4):
                    out[j] = total[:, j * width : (j + 1) * width]

            @pl.when(jnp.logical_not(first))
            def _():
                for j in range(4):
                    out[j] += total[:, j * width : (j + 1) * width]


def partials(saved_input, key_cot, value_cot, xs, zs, depth=512):
    count = xs.shape[0]
    tokens, features = saved_input.shape
    columns = key_cot.shape[1]
    width = features // (RING * RING)
    cot = pl.BlockSpec((depth, columns), lambda k, xs, zs: (k, 0))
    specs = [cot, cot]
    for i in range(count):
        for j in range(4):
            specs.append(
                pl.BlockSpec((depth, width), lambda k, xs, zs, i=i, j=j: (k, j * RING + xs[i]))
            )
        specs.append(pl.BlockSpec((depth, RING * width), lambda k, xs, zs, i=i: (k, zs[i])))
    shape = (RING, columns, width)
    outs = pl.pallas_call(
        functools.partial(partial_kernel, count, width),
        out_shape=[jax.ShapeDtypeStruct(shape, jnp.float32)] * (2 * count),
        grid_spec=pltpu.PrefetchScalarGridSpec(
            num_scalar_prefetch=2,
            grid=(tokens // depth,),
            in_specs=specs,
            out_specs=[pl.BlockSpec(shape, lambda k, xs, zs: (0, 0, 0))] * (2 * count),
        ),
        compiler_params=pltpu.CompilerParams(dimension_semantics=("arbitrary",)),
        cost_estimate=pl.CostEstimate(
            flops=4 * count * tokens * columns * RING * width,
            bytes_accessed=2 * tokens * (2 * columns + count * 2 * RING * width) + 8 * count * columns * RING * width,
            transcendentals=0,
        ),
        name="partials",
    )(xs, zs, key_cot, value_cot, *([saved_input] * (5 * count)))
    return [(outs[2 * i], outs[2 * i + 1]) for i in range(count)]


def gather(block, first, second):
    others = [shift(block, first, s) for s in (1, 2, 3)]
    line = jnp.stack([block, *others])
    before, after = shift(line, second, 1), shift(line, second, -1)
    far = shift(before[:2], second, 1), shift(after[2:], second, -1)
    return line, before, far[0], far[1], after


def pieces_of(refs):
    line, before, far_a, far_b, after = refs
    table = []
    for ref in (line, before, None, after):
        for s in range(4):
            if ref is None:
                table.append((far_a, s) if s < 2 else (far_b, s - 2))
            else:
                table.append((ref, s))
    return table


def block_rows(m, place, second, first):
    z, x = place
    if m == 0:
        return ((z + 4 - first) % 4) * 4 + (x + 4 - second) % 4
    return ((z + 4 - second) % 4) * 4 + (x + 4 - first) % 4


def raw_kernel(width, place_ref, left_ref, right_ref, *refs):
    pieces, (raw_ref, sums_ref) = refs[:10], refs[10:]
    place = place_ref[0], place_ref[1]
    rows = left_ref.shape[1]
    for m in range(2):
        table = pieces_of(pieces[m * 5 : m * 5 + 5])
        pre = None
        for second in range(4):
            for pair in range(2):
                lefts, rights = [], []
                for first in (2 * pair, 2 * pair + 1):
                    at_row = block_rows(m, place, second, first)
                    columns = pl.ds(pl.multiple_of(at_row * width, width), width)
                    lefts.append(left_ref[m, :, columns])
                    ref, j = table[second * 4 + first]
                    rights.append(ref[j])
                part = dot3(
                    split(jnp.concatenate(lefts, axis=1)),
                    split(jnp.concatenate(rights, axis=1)),
                    ((1,), (1,)),
                )
                pre = part if pre is None else pre + part
        raw = dot3(split(pre), split(right_ref[m]), ((1,), (0,)))
        raw_ref[m] = raw
        own = pieces[m * 5][0]
        sums_ref[m] = jnp.sum((own * own).reshape(-1, 8, width), axis=0)
        wide = raw * raw
        halves = wide[:, :width] + wide[:, width:]
        sums_ref[2 + m] = jnp.sum(halves.reshape(-1, 8, width), axis=0)


def stat_kernel(width, place_ref, left_ref, right_ref, *refs):
    pieces, (new_left_ref, new_right_ref) = refs[:10], refs[10:]
    place = place_ref[0], place_ref[1]
    for m in range(2):
        table = pieces_of(pieces[m * 5 : m * 5 + 5])
        own = split(pieces[m * 5][0])
        gram = None
        for second in range(4):
            for pair in range(2):
                rights, rows = [], []
                for first in (2 * pair, 2 * pair + 1):
                    rows.append(block_rows(m, place, second, first))
                    ref, j = table[second * 4 + first]
                    rights.append(ref[j])
                both = split(jnp.concatenate(rights, axis=1))
                part = dot3(both, both, ((1,), (1,)))
                gram = part if gram is None else gram + part
                left = dot3(own, both, ((0,), (0,)))
                for n in range(2):
                    columns = pl.ds(pl.multiple_of(rows[n] * width, width), width)
                    new_left_ref[m, :, columns] = (
                        decay_stat * left_ref[m, :, columns]
                        + (1.0 - decay_stat) * left[:, n * width : (n + 1) * width]
                    )
        new_right_ref[m] = decay_stat * right_ref[m] + (1.0 - decay_stat) * gram


def place_kernel(width, place_ref, *refs):
    pieces, out_ref = refs[:10], refs[10]
    place = place_ref[0], place_ref[1]
    for m in range(2):
        table = pieces_of(pieces[m * 5 : m * 5 + 5])
        for second in range(4):
            for first in range(4):
                ref, j = table[second * 4 + first]
                rows = pl.ds(pl.multiple_of(block_rows(m, place, second, first) * width, width), width)
                out_ref[m, rows, :] = ref[j]


def on_device(
    saved_input, key_cot, value_cot, weights, left_root, left_stat, right_root, right_stat
):
    rows = weights.shape[1]
    columns = weights.shape[2]
    z, x = lax.axis_index(Z), lax.axis_index(X)
    place = jnp.stack([z, x]).astype(jnp.int32)

    def offsets(me, *by):
        return jnp.stack([(me + b) % RING for b in by]).astype(jnp.int32)

    grads = functools.partial(partials, saved_input, key_cot, value_cot)
    ((ka, va),) = grads(offsets(x, 2), offsets(z, 2))
    first = [shift(ka[:2], X, 1), shift(ka[2:], X, -1), shift(va[:2], Z, 1), shift(va[2:], Z, -1)]
    (kb, vb), (kc, vc) = grads(offsets(x, 1, 3), offsets(z, 1, 3))
    second = [
        shift(jnp.concatenate([kb[:2] + first[0], kb[2:]]), X, 1),
        shift(jnp.concatenate([kc[:2], kc[2:] + first[1]]), X, -1),
        shift(jnp.concatenate([vb[:2] + first[2], vb[2:]]), Z, 1),
        shift(jnp.concatenate([vc[:2], vc[2:] + first[3]]), Z, -1),
    ]
    ((kd, vd),) = grads(offsets(x, 0), offsets(z, 0))

    def small(own, arrived_a, arrived_b, axis):
        me = lax.axis_index(axis)
        mine = [at(own, me + s) + at(arrived_a, me + s) + at(arrived_b, me + s) for s in range(4)]
        got = [shift(mine[s], axis, s) for s in (1, 2, 3)]
        return mine[0] + got[0] + (got[1] + got[2])

    keys = gather(small(kd, second[0], second[1], Z), Z, X)
    values = gather(small(vd, second[2], second[3], X), X, Z)
    pieces = [*keys, *values]

    block = right_root.shape[2]
    raw, sums = pl.pallas_call(
        functools.partial(raw_kernel, rows),
        out_shape=[
            jax.ShapeDtypeStruct((2, rows, columns), jnp.float32),
            jax.ShapeDtypeStruct((4, 8, rows), jnp.float32),
        ],
        in_specs=[SMEM] + [VMEM] * 12,
        out_specs=[VMEM, VMEM],
        name="raw",
    )(place, left_root[:, 0], right_root[:, 0], *pieces)

    sums = jnp.sum(sums, axis=(1, 2))
    everyone = lax.axis_size(FS_TP)
    spread = jnp.broadcast_to(jnp.pad(sums, (0, 124))[None, None], (everyone, 1, 128))
    sums = jnp.sum(lax.all_to_all(spread, FS_TP, 0, 0, tiled=True), axis=(0, 1))
    scale = jnp.sqrt(sums[:2] / (sums[2:4] + norm_eps))
    step = scale[:, None, None] * raw
    new_weights = weights - learn_rate * step
    narrow = new_weights.astype(jnp.bfloat16)
    copied = [*gather(narrow[0], Z, X), *gather(narrow[1], X, Z)]

    new_left, new_right = pl.pallas_call(
        functools.partial(stat_kernel, rows),
        out_shape=[
            jax.ShapeDtypeStruct((2, rows, rows * 16), jnp.float32),
            jax.ShapeDtypeStruct((2, block, block), jnp.float32),
        ],
        in_specs=[SMEM] + [VMEM] * 12,
        out_specs=[VMEM, VMEM],
        name="stats",
    )(place, left_stat[:, 0], right_stat[:, 0], *pieces)

    copies = pl.pallas_call(
        functools.partial(place_kernel, rows),
        out_shape=jax.ShapeDtypeStruct((2, rows * 16, columns), jnp.bfloat16),
        in_specs=[SMEM] + [VMEM] * 10,
        out_specs=VMEM,
        name="place",
    )(place, *copied)
    return (step, new_weights, copies, new_left[:, None], new_right[:, None])


def solution(mesh):
    split_mesh = Mesh(mesh.devices.reshape(4, 4, 4, 2), ("fs_0", "fs_1", "tp_0", "tp_1"))
    in_specs = (
        P(FS, None),
        P(FS, TP),
        P(FS, TP),
        P(None, FS, TP),
        P(None, TP, FS, None),
        P(None, TP, FS, None),
        P(None, TP, None, None),
        P(None, TP, None, None),
    )
    out_specs = (
        P(None, FS, TP),
        P(None, FS, TP),
        P(None, None, TP),
        P(None, TP, FS, None),
        P(None, TP, None, None),
    )
    return jax.shard_map(
        on_device, mesh=split_mesh, in_specs=in_specs, out_specs=out_specs, check_vma=False
    )
```

```python
import functools
import math

import jax
import jax.numpy as jnp
from jax import lax
from jax.experimental import pallas as pl
from jax.experimental.pallas import tpu as pltpu
from jax.sharding import Mesh
from jax.sharding import PartitionSpec as P

FS = ("fs_0", "fs_1")
FS_TP = ("fs_0", "fs_1", "tp_0", "tp_1")
TP = ("tp_0", "tp_1")
Z, X = FS
RING = 4
GROUPS = 16
SPAN = 250.0
FLOOR = 124.0
LN2 = math.log(2.0)
MIB = 1 << 20

decay_stat = 0.9
learn_rate = 0.05
norm_eps = 1e-06


VMEM = pl.BlockSpec(memory_space=pltpu.VMEM)
HBM = pl.BlockSpec(memory_space=pl.ANY)


def call(kernel, name, out_shape, in_specs, limit, scratch=()):
    single = not isinstance(out_shape, (list, tuple))
    return pl.pallas_call(
        kernel,
        out_shape=out_shape,
        in_specs=in_specs,
        out_specs=VMEM if single else [VMEM] * len(out_shape),
        scratch_shapes=list(scratch),
        compiler_params=pltpu.CompilerParams(vmem_limit_bytes=limit * MIB),
        name=name,
    )


def shift(value, axis, by):
    return lax.ppermute(value, axis, [(i, (i + by) % RING) for i in range(RING)])


def where_am_i():
    return lax.axis_index(Z), lax.axis_index(X)


def turn(index):
    return lax.rem(index, RING)


def lanes(index, width):
    return pl.ds(pl.multiple_of(index * width, width), width)


def encode(block, ref, j):
    columns, width = block.shape
    grouped = block.reshape(columns // GROUPS, GROUPS, width)
    size = jnp.abs(grouped)
    scale = (jnp.max(size, axis=0) * 1.0079 + 1e-30).astype(jnp.bfloat16)
    factor = SPAN / scale.astype(jnp.float32)
    code = jnp.exp2(size * factor[None] - FLOOR)
    code = jnp.where(grouped < 0.0, -code, code)
    ref[j, :columns, :] = code.reshape(columns, width).astype(jnp.bfloat16)
    ref[j, columns:, :] = scale


def decode(ref, j):
    rows, width = ref.shape[1:]
    columns = rows - GROUPS
    code = ref[j, :columns, :].astype(jnp.float32).reshape(columns // GROUPS, GROUPS, width)
    scale = ref[j, columns:, :].astype(jnp.float32) * (1.0 / (SPAN * LN2))
    size = (jnp.log(jnp.abs(code)) + FLOOR * LN2) * scale[None]
    return jnp.where(code < 0.0, -size, size).reshape(columns, width)


def split(value):
    high = value.astype(jnp.bfloat16)
    return high, (value - high.astype(jnp.float32)).astype(jnp.bfloat16)


def dot3(left, right, dims):
    (lh, ll), (rh, rl) = left, right
    dot = functools.partial(
        lax.dot_general, dimension_numbers=(dims, ((), ())), preferred_element_type=jnp.float32
    )
    return dot(lh, rh) + (dot(lh, rl) + dot(ll, rh))


def chunk(turned, x_ref, width, m, by):
    z, x = where_am_i()
    if m == 0:
        at = turn(x + by)
        columns = [x_ref[:, lanes(j * RING + at, width)] for j in range(RING)]
        columns = jnp.concatenate(columns, axis=1)
    else:
        columns = x_ref[:, lanes(turn(z + by), RING * width)]
    return jnp.dot(turned, columns, preferred_element_type=jnp.float32)


def coded_chunk(turned, x_ref, width, m, by, out):
    total = chunk(turned, x_ref, width, m, by)
    for j in range(RING):
        encode(total[:, j * width : (j + 1) * width], out, j)


def first_kernel(width, x_hbm, k_hbm, v_hbm, x_ref, kt_ref, vt_ref, out_k, out_v, k_ref, v_ref, sems):
    z, x = where_am_i()
    wide = RING * width
    parts = [(k_hbm, k_ref), (v_hbm, v_ref)]
    far = turn(z + 2)
    at = lanes(far, wide)
    parts.append((x_hbm.at[:, at], x_ref.at[:, at]))
    for by in (2, 1, 3, 0):
        for down in (1, 3, 0):
            at = lanes(turn(z + down) * RING + turn(x + by), width)
            parts.append((x_hbm.at[:, at], x_ref.at[:, at]))
    copies = [pltpu.make_async_copy(a, b, sems.at[i]) for i, (a, b) in enumerate(parts)]
    for c in copies:
        c.start()
    copies[0].wait()
    kt_ref[...] = k_ref[...].T
    copies[1].wait()
    vt_ref[...] = v_ref[...].T
    copies[2].wait()
    coded_chunk(vt_ref[...], x_ref, width, 1, 2, out_v)
    for c in copies[3:6]:
        c.wait()
    coded_chunk(kt_ref[...], x_ref, width, 0, 2, out_k)
    for c in copies[6:]:
        c.wait()


def near_kernel(width, x_ref, kt_ref, vt_ref, *outs):
    for i, (m, by) in enumerate(((0, 1), (1, 1), (0, 3), (1, 3))):
        coded_chunk((kt_ref, vt_ref)[m][...], x_ref, width, m, by, outs[i])


def own_kernel(width, x_ref, kt_ref, vt_ref, *outs):
    for m in range(2):
        total = chunk((kt_ref, vt_ref)[m][...], x_ref, width, m, 0)
        for j in range(RING):
            outs[m][j] = total[:, j * width : (j + 1) * width]


def sum_kernel(own_ref, a_ref, b_ref, c_ref, total_ref, code_ref):
    for j in range(RING):
        total = (own_ref[j] + decode(a_ref, j)) + (decode(b_ref, j) + decode(c_ref, j))
        total_ref[j] = total
        encode(total, code_ref, j)


def exchange(blocks, axis):
    return [shift(blocks, axis, s) for s in (2, 1, 3)]


OFFSETS = (2, 3, 1)


def gather(block, first, second):
    line = jnp.stack([block, *[shift(block, first, s) for s in (1, 2, 3)]])
    return [line, *exchange(line, second)]


def row_block(m, offset, j):
    z, x = where_am_i()
    if m == 0:
        return j * RING + turn(x + offset)
    return turn(z + offset) * RING + j


def raw_kernel(width, left_ref, right_ref, *refs):
    pieces, (raw_ref, sums_ref, halves_ref) = refs[:8], refs[8:]
    z, x = where_am_i()
    sums = []
    for m in range(2):
        pre = None
        for p, offset in enumerate((0, *OFFSETS)):
            ref = pieces[m * 4 + p]
            for pair in range(2):
                lefts, rights = [], []
                for j in (2 * pair, 2 * pair + 1):
                    lefts.append(left_ref[m, :, lanes(row_block(m, offset, j), width)])
                    rights.append(ref[j] if p == 0 else decode(ref, j))
                both = split(jnp.concatenate(rights, axis=1))
                halves_ref[m, p * 2 + pair, 0] = both[0]
                halves_ref[m, p * 2 + pair, 1] = both[1]
                part = dot3(split(jnp.concatenate(lefts, axis=1)), both, ((1,), (1,)))
                pre = part if pre is None else pre + part
        raw = dot3(split(pre), split(right_ref[m]), ((1,), (0,)))
        raw_ref[m] = raw
        own = pieces[m * 4][(z, x)[m]]
        sums.append((jnp.sum(own * own), jnp.sum(raw * raw)))
    lane = lax.broadcasted_iota(jnp.int32, (1, 128), 1)
    left = jnp.where(lane < 32, sums[0][0], sums[1][0])
    right = jnp.where(lane < 96, sums[0][1], sums[1][1])
    sums_ref[...] = jnp.where(lane < 64, left, right)


def weight_kernel(sums_ref, raw_ref, weights_ref, step_ref, new_ref, *narrow):
    total = jnp.sum(sums_ref[...], axis=0, keepdims=True)
    for m in range(2):
        grad_sq = total[:, m * 32 : m * 32 + 1]
        raw_sq = total[:, 64 + m * 32 : 64 + m * 32 + 1]
        step = jnp.sqrt(grad_sq / (raw_sq + norm_eps)) * raw_ref[m]
        new = weights_ref[m] - learn_rate * step
        step_ref[m] = step
        new_ref[m] = new
        narrow[m][...] = new.astype(jnp.bfloat16)


def stat_kernel(width, left_ref, right_ref, line_k, line_v, halves_ref, new_left_ref, new_right_ref):
    z, x = where_am_i()
    for m in range(2):
        own = split((line_k, line_v)[m][(z, x)[m]])
        gram = None
        for p, offset in enumerate((0, *OFFSETS)):
            for pair in range(2):
                both = halves_ref[m, p * 2 + pair, 0], halves_ref[m, p * 2 + pair, 1]
                part = dot3(both, both, ((1,), (1,)))
                gram = part if gram is None else gram + part
                left = dot3(own, both, ((0,), (0,)))
                for n in range(2):
                    at = lanes(row_block(m, offset, 2 * pair + n), width)
                    new_left_ref[m, :, at] = (
                        decay_stat * left_ref[m, :, at]
                        + (1.0 - decay_stat) * left[:, n * width : (n + 1) * width]
                    )
        new_right_ref[m] = decay_stat * right_ref[m] + (1.0 - decay_stat) * gram


def place_kernel(width, *refs):
    pieces, out_ref = refs[:8], refs[8]
    z, x = where_am_i()
    for m in range(2):
        for p, offset in enumerate((0, *OFFSETS)):
            for back in range(RING):
                j = turn((z, x)[m] + RING - back)
                out_ref[m, lanes(row_block(m, offset, j), width), :] = pieces[m * 4 + p][back]


def on_device(
    saved_input, key_cot, value_cot, weights, left_root, left_stat, right_root, right_stat
):
    tokens, features = saved_input.shape
    rows, columns = weights.shape[1:]
    f32, bf16 = jnp.float32, jnp.bfloat16
    blocks = (RING, columns, rows)
    coded = (RING, columns + GROUPS, rows)

    x_here, kt, vt, k2, v2 = call(
        functools.partial(first_kernel, rows),
        "first",
        [
            pltpu.VMEM((tokens, features), bf16),
            pltpu.VMEM((columns, tokens), bf16),
            pltpu.VMEM((columns, tokens), bf16),
            pltpu.VMEM(coded, bf16),
            pltpu.VMEM(coded, bf16),
        ],
        [HBM] * 3,
        16,
        [
            pltpu.VMEM((tokens, columns), bf16),
            pltpu.VMEM((tokens, columns), bf16),
            pltpu.SemaphoreType.DMA((15,)),
        ],
    )(*[pltpu.with_memory_space_constraint(a, pltpu.HBM) for a in (saved_input, key_cot, value_cot)])
    k2, v2 = shift(k2, X, 2), shift(v2, Z, 2)
    k1, v1, k3, v3 = call(
        functools.partial(near_kernel, rows), "near", [pltpu.VMEM(coded, bf16)] * 4, [VMEM] * 3, 12
    )(x_here, kt, vt)
    k1, v1, k3, v3 = shift(k1, X, 1), shift(v1, Z, 1), shift(k3, X, 3), shift(v3, Z, 3)
    k0, v0 = call(
        functools.partial(own_kernel, rows), "own", [pltpu.VMEM(blocks, f32)] * 2, [VMEM] * 3, 12
    )(x_here, kt, vt)

    add = call(
        sum_kernel, "sum", [pltpu.VMEM(blocks, f32), pltpu.VMEM(coded, bf16)], [VMEM] * 4, 16
    )
    k0, code_k = add(k0, k2, k1, k3)
    got_k = exchange(code_k, Z)
    v0, code_v = add(v0, v2, v1, v3)
    got_v = exchange(code_v, X)
    line_k, code_k = add(k0, *got_k)
    pieces_k = exchange(code_k, X)
    line_v, code_v = add(v0, *got_v)
    pieces_v = exchange(code_v, Z)

    raw, sums, halves = call(
        functools.partial(raw_kernel, rows),
        "raw",
        [
            pltpu.VMEM((2, rows, columns), f32),
            pltpu.VMEM((1, 128), f32),
            pltpu.VMEM((2, 2 * RING, 2, columns, 2 * rows), bf16),
        ],
        [VMEM] * 10,
        20,
    )(left_root[:, 0], right_root[:, 0], line_k, *pieces_k, line_v, *pieces_v)

    everyone = lax.axis_size(FS_TP)
    spread = jnp.broadcast_to(sums[None], (everyone, 1, 128))
    sums = lax.all_to_all(spread, FS_TP, 0, 0, tiled=True).reshape(everyone, 128)
    step, new_weights, narrow_k, narrow_v = call(
        weight_kernel,
        "weights",
        [
            jax.ShapeDtypeStruct(weights.shape, f32),
            jax.ShapeDtypeStruct(weights.shape, f32),
            pltpu.VMEM((rows, columns), bf16),
            pltpu.VMEM((rows, columns), bf16),
        ],
        [VMEM] * 3,
        8,
    )(sums, raw, weights)
    copied = [*gather(narrow_k, Z, X), *gather(narrow_v, X, Z)]

    new_left, new_right = call(
        functools.partial(stat_kernel, rows),
        "stats",
        [
            jax.ShapeDtypeStruct((2, rows, features), f32),
            jax.ShapeDtypeStruct((2, columns, columns), f32),
        ],
        [VMEM] * 5,
        20,
    )(left_stat[:, 0], right_stat[:, 0], line_k, line_v, halves)

    copies = call(
        functools.partial(place_kernel, rows),
        "place",
        jax.ShapeDtypeStruct((2, features, columns), bf16),
        [VMEM] * 8,
        12,
    )(*copied)
    return (step, new_weights, copies, new_left[:, None], new_right[:, None])


def solution(mesh):
    rings = Mesh(mesh.devices.reshape(4, 4, 4, 2), ("fs_0", "fs_1", "tp_0", "tp_1"))
    in_specs = (
        P(FS, None),
        P(FS, TP),
        P(FS, TP),
        P(None, FS, TP),
        P(None, TP, FS, None),
        P(None, TP, FS, None),
        P(None, TP, None, None),
        P(None, TP, None, None),
    )
    out_specs = (
        P(None, FS, TP),
        P(None, FS, TP),
        P(None, None, TP),
        P(None, TP, FS, None),
        P(None, TP, None, None),
    )
    return jax.shard_map(
        on_device, mesh=rings, in_specs=in_specs, out_specs=out_specs, check_vma=False
    )
```

```python
import functools
import math

import jax
import jax.numpy as jnp
from jax import lax
from jax.experimental import pallas as pl
from jax.experimental.pallas import tpu as pltpu
from jax.sharding import Mesh
from jax.sharding import PartitionSpec as P


FS = ("fs_0", "fs_1")
FS_TP = ("fs_0", "fs_1", "tp_0", "tp_1")
TP = ("tp_0", "tp_1")
Z, X = FS
RING = 4
GROUPS = 8
SPAN = 250.0
FLOOR = 124.0
LN2 = math.log(2.0)
MIB = 1 << 20

decay_stat = 0.9
learn_rate = 0.05
norm_eps = 1e-06


VMEM = pl.BlockSpec(memory_space=pltpu.VMEM)
HBM = pl.BlockSpec(memory_space=pl.ANY)


def call(kernel, out_shape, in_specs, limit, scratch=(), out_specs=None, aliases=None):
    single = not isinstance(out_shape, (list, tuple))
    if out_specs is None:
        out_specs = VMEM if single else [VMEM] * len(out_shape)
    return pl.pallas_call(
        kernel,
        out_shape=out_shape,
        in_specs=in_specs,
        out_specs=out_specs,
        scratch_shapes=list(scratch),
        input_output_aliases=aliases or {},
        compiler_params=pltpu.CompilerParams(vmem_limit_bytes=limit * MIB),
    )


def shift(value, axis, by):
    return lax.ppermute(value, axis, [(i, (i + by) % RING) for i in range(RING)])


def where_am_i():
    return lax.axis_index(Z), lax.axis_index(X)


def turn(index):
    return lax.rem(index, RING)


def lanes(index, width):
    return pl.ds(pl.multiple_of(index * width, width), width)


def encode(block, ref, j):
    columns, width = block.shape
    grouped = block.reshape(columns // GROUPS, GROUPS, width)
    size = jnp.abs(grouped)
    scale = (jnp.max(size, axis=0) * 1.0079 + 1e-30).astype(jnp.bfloat16)
    factor = SPAN / scale.astype(jnp.float32)
    code = jnp.exp2(size * factor[None] - FLOOR)
    code = jnp.where(grouped < 0.0, -code, code)
    ref[j, :columns, :] = code.reshape(columns, width).astype(jnp.bfloat16)
    ref[j, columns:, :] = scale


def decode(ref, j):
    rows, width = ref.shape[1:]
    columns = rows - GROUPS
    code = ref[j, :columns, :].astype(jnp.float32).reshape(columns // GROUPS, GROUPS, width)
    scale = ref[j, columns:, :].astype(jnp.float32) * (1.0 / (SPAN * LN2))
    size = (jnp.log(jnp.abs(code)) + FLOOR * LN2) * scale[None]
    return jnp.where(code < 0.0, -size, size).reshape(columns, width)


def split(value):
    high = value.astype(jnp.bfloat16)
    return high, (value - high.astype(jnp.float32)).astype(jnp.bfloat16)


def dot3(left, right, dims):
    (lh, ll), (rh, rl) = left, right
    dot = functools.partial(
        lax.dot_general, dimension_numbers=(dims, ((), ())), preferred_element_type=jnp.float32
    )
    return dot(lh, rh) + (dot(lh, rl) + dot(ll, rh))


def chunk(turned, x_ref, width, m, by):
    z, x = where_am_i()
    if m == 0:
        at = turn(x + by)
        columns = [x_ref[:, lanes(j * RING + at, width)] for j in range(RING)]
        columns = jnp.concatenate(columns, axis=1)
    else:
        columns = x_ref[:, lanes(turn(z + by), RING * width)]
    return jnp.dot(turned, columns, preferred_element_type=jnp.float32)


def coded_chunk(turned, x_ref, width, m, by, out):
    total = chunk(turned, x_ref, width, m, by)
    for j in range(RING):
        encode(total[:, j * width : (j + 1) * width], out, j)


def columns_of(x_hbm, x_ref, width, down, by):
    z, x = where_am_i()
    at = lanes(turn(z + down) * RING + turn(x + by), width)
    return x_hbm.at[:, at], x_ref.at[:, at]


def started(parts, sems):
    copies = [pltpu.make_async_copy(a, b, sems.at[i]) for i, (a, b) in enumerate(parts)]
    for c in copies:
        c.start()
    return copies


def first_kernel(width, x_hbm, k_hbm, v_hbm, x_ref, kt_ref, vt_ref, out_k, out_v, k_ref, v_ref, sems):
    z, _ = where_am_i()
    at = lanes(turn(z + 2), RING * width)
    parts = [(v_hbm, v_ref), (x_hbm.at[:, at], x_ref.at[:, at]), (k_hbm, k_ref)]
    for by in (2, 1, 3, 0):
        parts += [columns_of(x_hbm, x_ref, width, down, by) for down in (1, 3, 0)]
    copies = started(parts, sems)
    copies[0].wait()
    vt_ref[...] = v_ref[...].T
    copies[1].wait()
    coded_chunk(vt_ref[...], x_ref, width, 1, 2, out_v)
    copies[2].wait()
    kt_ref[...] = k_ref[...].T
    for c in copies[3:6]:
        c.wait()
    coded_chunk(kt_ref[...], x_ref, width, 0, 2, out_k)
    for c in copies[6:]:
        c.wait()


def near_kernel(width, x_ref, kt_ref, vt_ref, *outs):
    for i, (m, by) in enumerate(((0, 1), (1, 1), (0, 3), (1, 3))):
        coded_chunk((kt_ref, vt_ref)[m][...], x_ref, width, m, by, outs[i])


def own_kernel(width, x_ref, kt_ref, vt_ref, *outs):
    for m in range(2):
        total = chunk((kt_ref, vt_ref)[m][...], x_ref, width, m, 0)
        for j in range(RING):
            outs[m][j] = total[:, j * width : (j + 1) * width]


def sum_kernel(own_ref, a_ref, b_ref, c_ref, total_ref, code_ref):
    for j in range(RING):
        total = (own_ref[j] + decode(a_ref, j)) + (decode(b_ref, j) + decode(c_ref, j))
        total_ref[j] = total
        encode(total, code_ref, j)


def exchange(blocks, axis):
    return [shift(blocks, axis, s) for s in (2, 1, 3)]


OFFSETS = (2, 3, 1)


def gather(block, first, second):
    line = jnp.stack([block, *[shift(block, first, s) for s in (1, 2, 3)]])
    return [line, *exchange(line, second)]


def row_block(m, offset, j):
    z, x = where_am_i()
    if m == 0:
        return j * RING + turn(x + offset)
    return turn(z + offset) * RING + j


def raw_kernel(width, m, left_ref, right_ref, before_ref, line_ref, a_ref, b_ref, c_ref, raw_ref, sums_ref, halves_ref):
    pre = None
    for p, (offset, ref) in enumerate(zip((0, *OFFSETS), (line_ref, a_ref, b_ref, c_ref))):
        for pair in range(2):
            lefts, rights = [], []
            for j in (2 * pair, 2 * pair + 1):
                lefts.append(left_ref[m, :, lanes(row_block(m, offset, j), width)])
                rights.append(ref[j] if p == 0 else decode(ref, j))
            both = split(jnp.concatenate(rights, axis=1))
            halves_ref[p * 2 + pair, 0] = both[0]
            halves_ref[p * 2 + pair, 1] = both[1]
            part = dot3(split(jnp.concatenate(lefts, axis=1)), both, ((1,), (1,)))
            pre = part if pre is None else pre + part
    raw = dot3(split(pre), split(right_ref[m]), ((1,), (0,)))
    raw_ref[...] = raw
    own = line_ref[where_am_i()[m]]
    lane = lax.broadcasted_iota(jnp.int32, (1, 128), 1)
    mine = jnp.where(lane < 64, jnp.sum(own * own), jnp.sum(raw * raw))
    sums_ref[...] = jnp.where((lane // 32) % 2 == m, mine, before_ref[...])


def weight_kernel(sums_ref, raw_k, raw_v, weights_ref, step_ref, new_ref, *narrow):
    total = jnp.sum(sums_ref[...], axis=0, keepdims=True)
    for m in range(2):
        grad_sq = total[:, m * 32 : m * 32 + 1]
        raw_sq = total[:, 64 + m * 32 : 64 + m * 32 + 1]
        step = jnp.sqrt(grad_sq / (raw_sq + norm_eps)) * (raw_k, raw_v)[m][...]
        new = weights_ref[m] - learn_rate * step
        step_ref[m] = step
        new_ref[m] = new
        narrow[m][...] = new.astype(jnp.bfloat16)


def stat_kernel(width, left_ref, right_ref, line_k, line_v, halves_k, halves_v, new_left_ref, new_right_ref):
    z, x = where_am_i()
    for m in range(2):
        own = split((line_k, line_v)[m][(z, x)[m]])
        gram = None
        for p, offset in enumerate((0, *OFFSETS)):
            for pair in range(2):
                halves = (halves_k, halves_v)[m]
                both = halves[p * 2 + pair, 0], halves[p * 2 + pair, 1]
                part = dot3(both, both, ((1,), (1,)))
                gram = part if gram is None else gram + part
                left = dot3(own, both, ((0,), (0,)))
                for n in range(2):
                    at = lanes(row_block(m, offset, 2 * pair + n), width)
                    new_left_ref[m, :, at] = (
                        decay_stat * left_ref[m, :, at]
                        + (1.0 - decay_stat) * left[:, n * width : (n + 1) * width]
                    )
        new_right_ref[m] = decay_stat * right_ref[m] + (1.0 - decay_stat) * gram


def place_kernel(width, *refs):
    pieces, out_ref, sems = refs[:-2], refs[-2], refs[-1]
    parts = []
    for m in range(2):
        me = where_am_i()[m]
        for piece, offset in zip(pieces[m * RING :], (0, *OFFSETS)):
            for back in range(RING):
                at = row_block(m, offset, turn(me + RING - back)) * width
                rows = pl.ds(pl.multiple_of(at, width), width)
                parts.append((piece.at[back], out_ref.at[m, rows, :]))
    for c in started(parts, sems):
        c.wait()


def on_device(
    saved_input, key_cot, value_cot, weights, left_root, left_stat, right_root, right_stat
):
    tokens, features = saved_input.shape
    rows, columns = weights.shape[1:]
    f32, bf16 = jnp.float32, jnp.bfloat16
    blocks = (RING, columns, rows)
    coded = (RING, columns + GROUPS, rows)

    x_hbm, k_hbm, v_hbm = [
        pltpu.with_memory_space_constraint(a, pltpu.HBM) for a in (saved_input, key_cot, value_cot)
    ]
    x_here, kt, vt, k2, v2 = call(
        functools.partial(first_kernel, rows),
        [
            pltpu.VMEM((tokens, features), bf16),
            pltpu.VMEM((columns, tokens), bf16),
            pltpu.VMEM((columns, tokens), bf16),
            pltpu.VMEM(coded, bf16),
            pltpu.VMEM(coded, bf16),
        ],
        [HBM] * 3,
        16,
        [
            pltpu.VMEM((tokens, columns), bf16),
            pltpu.VMEM((tokens, columns), bf16),
            pltpu.SemaphoreType.DMA((15,)),
        ],
    )(x_hbm, k_hbm, v_hbm)
    v2, k2 = shift(v2, Z, 2), shift(k2, X, 2)
    k1, v1, k3, v3 = call(
        functools.partial(near_kernel, rows), [pltpu.VMEM(coded, bf16)] * 4, [VMEM] * 3, 12
    )(x_here, kt, vt)
    k1, v1, k3, v3 = shift(k1, X, 1), shift(v1, Z, 1), shift(k3, X, 3), shift(v3, Z, 3)
    k0, v0 = call(
        functools.partial(own_kernel, rows), [pltpu.VMEM(blocks, f32)] * 2, [VMEM] * 3, 12
    )(x_here, kt, vt)

    add = call(sum_kernel, [pltpu.VMEM(blocks, f32), pltpu.VMEM(coded, bf16)], [VMEM] * 4, 16)
    v0, code_v = add(v0, v2, v1, v3)
    got_v = exchange(code_v, X)
    k0, code_k = add(k0, k2, k1, k3)
    got_k = exchange(code_k, Z)
    line_v, code_v = add(v0, *got_v)
    pieces_v = exchange(code_v, Z)
    line_k, code_k = add(k0, *got_k)
    pieces_k = exchange(code_k, X)

    def direction(m, before, line, pieces):
        return call(
            functools.partial(raw_kernel, rows, m),
            [
                pltpu.VMEM((rows, columns), f32),
                pltpu.VMEM((1, 128), f32),
                pltpu.VMEM((2 * RING, 2, columns, 2 * rows), bf16),
            ],
            [VMEM] * 7,
            12,
        )(left_root[:, 0], right_root[:, 0], before, line, *pieces)

    raw_v, sums, halves_v = direction(1, jnp.zeros((1, 128), f32), line_v, pieces_v)
    raw_k, sums, halves_k = direction(0, sums, line_k, pieces_k)

    everyone = lax.axis_size(FS_TP)
    spread = jnp.broadcast_to(sums[None], (everyone, 1, 128))
    sums = lax.all_to_all(spread, FS_TP, 0, 0, tiled=True).reshape(everyone, 128)
    step, new_weights, narrow_k, narrow_v = call(
        weight_kernel,
        [
            jax.ShapeDtypeStruct(weights.shape, f32),
            jax.ShapeDtypeStruct(weights.shape, f32),
            pltpu.VMEM((rows, columns), bf16),
            pltpu.VMEM((rows, columns), bf16),
        ],
        [VMEM] * 4,
        8,
    )(sums, raw_k, raw_v, weights)
    copied = gather(narrow_k, Z, X), gather(narrow_v, X, Z)

    new_left, new_right = call(
        functools.partial(stat_kernel, rows),
        [
            jax.ShapeDtypeStruct((2, rows, features), f32),
            jax.ShapeDtypeStruct((2, columns, columns), f32),
        ],
        [VMEM] * 6,
        20,
    )(left_stat[:, 0], right_stat[:, 0], line_k, line_v, halves_k, halves_v)

    copies = call(
        functools.partial(place_kernel, rows),
        jax.ShapeDtypeStruct((2, features, columns), bf16),
        [VMEM] * 8,
        4,
        [pltpu.SemaphoreType.DMA((32,))],
        out_specs=HBM,
    )(*copied[0], *copied[1])
    return (step, new_weights, copies, new_left[:, None], new_right[:, None])


def solution(mesh):
    rings = Mesh(mesh.devices.reshape(4, 4, 4, 2), ("fs_0", "fs_1", "tp_0", "tp_1"))
    in_specs = (
        P(FS, None),
        P(FS, TP),
        P(FS, TP),
        P(None, FS, TP),
        P(None, TP, FS, None),
        P(None, TP, FS, None),
        P(None, TP, None, None),
        P(None, TP, None, None),
    )
    out_specs = (
        P(None, FS, TP),
        P(None, FS, TP),
        P(None, None, TP),
        P(None, TP, FS, None),
        P(None, TP, None, None),
    )

    return jax.shard_map(
        on_device, mesh=rings, in_specs=in_specs, out_specs=out_specs, check_vma=False
    )
```

```python
import functools
import math

import jax
import jax.numpy as jnp
from jax import lax
from jax.experimental import pallas as pl
from jax.experimental.pallas import tpu as pltpu
from jax.sharding import Mesh
from jax.sharding import PartitionSpec as P


FS = ("fs_0", "fs_1")
FS_TP = ("fs_0", "fs_1", "tp_0", "tp_1")
TP = ("tp_0", "tp_1")
Z, X = FS
RING = 4
GROUPS = 8
SPAN = 250.0
FLOOR = 124.0
LN2 = math.log(2.0)
MIB = 1 << 20

decay_stat = 0.9
learn_rate = 0.05
norm_eps = 1e-06


VMEM = pl.BlockSpec(memory_space=pltpu.VMEM)
HBM = pl.BlockSpec(memory_space=pl.ANY)


def call(kernel, out_shape, in_specs, limit, scratch=(), out_specs=None, aliases=None):
    single = not isinstance(out_shape, (list, tuple))
    if out_specs is None:
        out_specs = VMEM if single else [VMEM] * len(out_shape)
    return pl.pallas_call(
        kernel,
        out_shape=out_shape,
        in_specs=in_specs,
        out_specs=out_specs,
        scratch_shapes=list(scratch),
        input_output_aliases=aliases or {},
        compiler_params=pltpu.CompilerParams(vmem_limit_bytes=limit * MIB),
    )


def shift(value, axis, by):
    return lax.ppermute(value, axis, [(i, (i + by) % RING) for i in range(RING)])


def where_am_i():
    return lax.axis_index(Z), lax.axis_index(X)


def turn(index):
    return lax.rem(index, RING)


def lanes(index, width):
    return pl.ds(pl.multiple_of(index * width, width), width)


def encode(block, ref, j):
    columns, width = block.shape
    grouped = block.reshape(columns // GROUPS, GROUPS, width)
    size = jnp.abs(grouped)
    scale = (jnp.max(size, axis=0) * 1.0079 + 1e-30).astype(jnp.bfloat16)
    factor = SPAN / scale.astype(jnp.float32)
    code = jnp.exp2(size * factor[None] - FLOOR)
    code = jnp.where(grouped < 0.0, -code, code)
    ref[j, :columns, :] = code.reshape(columns, width).astype(jnp.bfloat16)
    ref[j, columns:, :] = scale


def decode(ref, j):
    rows, width = ref.shape[1:]
    columns = rows - GROUPS
    code = ref[j, :columns, :].astype(jnp.float32).reshape(columns // GROUPS, GROUPS, width)
    scale = ref[j, columns:, :].astype(jnp.float32) * (1.0 / (SPAN * LN2))
    size = (jnp.log(jnp.abs(code)) + FLOOR * LN2) * scale[None]
    return jnp.where(code < 0.0, -size, size).reshape(columns, width)


def split(value):
    high = value.astype(jnp.bfloat16)
    return high, (value - high.astype(jnp.float32)).astype(jnp.bfloat16)


def dot3(left, right, dims):
    (lh, ll), (rh, rl) = left, right
    dot = functools.partial(
        lax.dot_general, dimension_numbers=(dims, ((), ())), preferred_element_type=jnp.float32
    )
    return dot(lh, rh) + (dot(lh, rl) + dot(ll, rh))


def chunk(turned, x_ref, width, m, by):
    z, x = where_am_i()
    if m == 0:
        at = turn(x + by)
        columns = [x_ref[:, lanes(j * RING + at, width)] for j in range(RING)]
        columns = jnp.concatenate(columns, axis=1)
    else:
        columns = x_ref[:, lanes(turn(z + by), RING * width)]
    return jnp.dot(turned, columns, preferred_element_type=jnp.float32)


def coded_chunk(turned, x_ref, width, m, by, out):
    total = chunk(turned, x_ref, width, m, by)
    for j in range(RING):
        encode(total[:, j * width : (j + 1) * width], out, j)


def columns_of(x_hbm, x_ref, width, down, by):
    z, x = where_am_i()
    at = lanes(turn(z + down) * RING + turn(x + by), width)
    return x_hbm.at[:, at], x_ref.at[:, at]


def started(parts, sems):
    copies = [pltpu.make_async_copy(a, b, sems.at[i]) for i, (a, b) in enumerate(parts)]
    for c in copies:
        c.start()
    return copies


def first_kernel(width, x_hbm, k_hbm, v_hbm, x_ref, kt_ref, vt_ref, out_k, out_v, k_ref, v_ref, sems):
    z, _ = where_am_i()
    at = lanes(turn(z + 2), RING * width)
    parts = [(v_hbm, v_ref), (k_hbm, k_ref), (x_hbm.at[:, at], x_ref.at[:, at])]
    for by in (2, 1, 3, 0):
        parts += [columns_of(x_hbm, x_ref, width, down, by) for down in (1, 3, 0)]
    copies = started(parts, sems)
    copies[0].wait()
    vt_ref[...] = v_ref[...].T
    copies[1].wait()
    kt_ref[...] = k_ref[...].T
    copies[2].wait()
    coded_chunk(vt_ref[...], x_ref, width, 1, 2, out_v)
    for c in copies[3:6]:
        c.wait()
    coded_chunk(kt_ref[...], x_ref, width, 0, 2, out_k)
    for c in copies[6:]:
        c.wait()


def near_kernel(width, x_ref, kt_ref, vt_ref, *outs):
    for i, (m, by) in enumerate(((1, 1), (0, 1), (1, 3), (0, 3))):
        coded_chunk((kt_ref, vt_ref)[m][...], x_ref, width, m, by, outs[i])


def own_kernel(width, x_ref, kt_ref, vt_ref, *outs):
    for m in range(2):
        total = chunk((kt_ref, vt_ref)[m][...], x_ref, width, m, 0)
        for j in range(RING):
            outs[m][j] = total[:, j * width : (j + 1) * width]


def sum_kernel(own_ref, a_ref, b_ref, c_ref, total_ref, code_ref):
    for j in range(RING):
        total = (own_ref[j] + decode(a_ref, j)) + (decode(b_ref, j) + decode(c_ref, j))
        total_ref[j] = total
        encode(total, code_ref, j)


def exchange(blocks, axis):
    return [shift(blocks, axis, s) for s in (2, 1, 3)]


OFFSETS = (2, 3, 1)


def row_block(m, offset, j):
    z, x = where_am_i()
    if m == 0:
        return j * RING + turn(x + offset)
    return turn(z + offset) * RING + j


def raw_kernel(width, m, left_ref, right_ref, before_ref, weights_ref, line_ref, a_ref, b_ref, c_ref, raw_ref, sums_ref, halves_ref):
    pre = None
    for p, (offset, ref) in enumerate(zip((0, *OFFSETS), (line_ref, a_ref, b_ref, c_ref))):
        for pair in range(2):
            lefts, rights = [], []
            for j in (2 * pair, 2 * pair + 1):
                lefts.append(left_ref[m, :, lanes(row_block(m, offset, j), width)])
                rights.append(ref[j] if p == 0 else decode(ref, j))
            both = split(jnp.concatenate(rights, axis=1))
            halves_ref[p * 2 + pair, 0] = both[0]
            halves_ref[p * 2 + pair, 1] = both[1]
            part = dot3(split(jnp.concatenate(lefts, axis=1)), both, ((1,), (1,)))
            pre = part if pre is None else pre + part
    raw = dot3(split(pre), split(right_ref[m]), ((1,), (0,)))
    raw_ref[0] = raw
    raw_ref[1] = weights_ref[m]
    own = line_ref[where_am_i()[m]]
    lane = lax.broadcasted_iota(jnp.int32, (1, 128), 1)
    mine = jnp.where(lane < 64, jnp.sum(own * own), jnp.sum(raw * raw))
    sums_ref[...] = jnp.where((lane // 32) % 2 == m, mine, before_ref[...])


def weight_kernel(sums_ref, *refs):
    ins, (step_ref, new_ref, *lines) = refs[: 2 * RING], refs[2 * RING :]
    total = jnp.sum(sums_ref[...], axis=0, keepdims=True)
    for m in range(2):
        grad_sq = total[:, m * 32 : m * 32 + 1]
        raw_sq = total[:, 64 + m * 32 : 64 + m * 32 + 1]
        scale = jnp.sqrt(grad_sq / (raw_sq + norm_eps))
        for back in range(RING):
            ref = ins[m * RING + back]
            step = scale * ref[0]
            new = ref[1] - learn_rate * step
            if back == 0:
                step_ref[m] = step
                new_ref[m] = new
            lines[m][back] = new.astype(jnp.bfloat16)


def stat_kernel(width, left_ref, right_ref, line_k, line_v, halves_k, halves_v, new_left_ref, new_right_ref):
    z, x = where_am_i()
    for m in range(2):
        own = split((line_k, line_v)[m][(z, x)[m]])
        gram = None
        for p, offset in enumerate((0, *OFFSETS)):
            for pair in range(2):
                halves = (halves_k, halves_v)[m]
                both = halves[p * 2 + pair, 0], halves[p * 2 + pair, 1]
                part = dot3(both, both, ((1,), (1,)))
                gram = part if gram is None else gram + part
                left = dot3(own, both, ((0,), (0,)))
                for n in range(2):
                    at = lanes(row_block(m, offset, 2 * pair + n), width)
                    new_left_ref[m, :, at] = (
                        decay_stat * left_ref[m, :, at]
                        + (1.0 - decay_stat) * left[:, n * width : (n + 1) * width]
                    )
        new_right_ref[m] = decay_stat * right_ref[m] + (1.0 - decay_stat) * gram


def place_kernel(width, chosen, *refs):
    out_ref, sems = refs[-2:]
    parts = []
    for piece, (m, p) in zip(refs, chosen):
        me, offset = where_am_i()[1 - m], (0, *OFFSETS)[p]
        for back in range(RING):
            at = row_block(1 - m, offset, turn(me + RING - back)) * width
            rows = pl.ds(pl.multiple_of(at, width), width)
            parts.append((piece.at[back], out_ref.at[m, rows, :]))
    for c in started(parts, sems):
        c.wait()


def on_device(
    saved_input, key_cot, value_cot, weights, left_root, left_stat, right_root, right_stat
):
    tokens, features = saved_input.shape
    rows, columns = weights.shape[1:]
    f32, bf16 = jnp.float32, jnp.bfloat16
    blocks = (RING, columns, rows)
    coded = (RING, columns + GROUPS, rows)

    x_hbm, k_hbm, v_hbm = [
        pltpu.with_memory_space_constraint(a, pltpu.HBM) for a in (saved_input, key_cot, value_cot)
    ]
    x_here, kt, vt, k2, v2 = call(
        functools.partial(first_kernel, rows),
        [
            pltpu.VMEM((tokens, features), bf16),
            pltpu.VMEM((columns, tokens), bf16),
            pltpu.VMEM((columns, tokens), bf16),
            pltpu.VMEM(coded, bf16),
            pltpu.VMEM(coded, bf16),
        ],
        [HBM] * 3,
        16,
        [
            pltpu.VMEM((tokens, columns), bf16),
            pltpu.VMEM((tokens, columns), bf16),
            pltpu.SemaphoreType.DMA((15,)),
        ],
    )(x_hbm, k_hbm, v_hbm)
    v2, k2 = shift(v2, Z, 2), shift(k2, X, 2)
    v1, k1, v3, k3 = call(
        functools.partial(near_kernel, rows), [pltpu.VMEM(coded, bf16)] * 4, [VMEM] * 3, 12
    )(x_here, kt, vt)
    v1, k1 = shift(v1, Z, 1), shift(k1, X, 1)
    v3, k3 = shift(v3, Z, 3), shift(k3, X, 3)
    k0, v0 = call(functools.partial(own_kernel, rows), [pltpu.VMEM(blocks, f32)] * 2, [VMEM] * 3, 12)(x_here, kt, vt)

    add = call(sum_kernel, [pltpu.VMEM(blocks, f32), pltpu.VMEM(coded, bf16)], [VMEM] * 4, 16)
    v0, code_v = add(v0, v2, v1, v3)
    got_v = exchange(code_v, X)
    k0, code_k = add(k0, k2, k1, k3)
    got_k = exchange(code_k, Z)
    line_v, code_v = add(v0, *got_v)
    pieces_v = exchange(code_v, Z)
    line_k, code_k = add(k0, *got_k)
    pieces_k = exchange(code_k, X)

    def direction(m, before, line, pieces):
        return call(
            functools.partial(raw_kernel, rows, m),
            [
                pltpu.VMEM((2, rows, columns), f32),
                pltpu.VMEM((1, 128), f32),
                pltpu.VMEM((2 * RING, 2, columns, 2 * rows), bf16),
            ],
            [VMEM] * 8,
            12,
        )(left_root[:, 0], right_root[:, 0], before, weights, line, *pieces)

    value, sums, halves_v = direction(1, jnp.zeros((1, 128), f32), line_v, pieces_v)
    values = [value, *[shift(value, Z, s) for s in (1, 2, 3)]]
    key, sums, halves_k = direction(0, sums, line_k, pieces_k)
    keys = [key, *[shift(key, X, s) for s in (1, 2, 3)]]

    everyone = lax.axis_size(FS_TP)
    spread = jnp.broadcast_to(sums[None], (everyone, 1, 128))
    sums = lax.all_to_all(spread, FS_TP, 0, 0, tiled=True).reshape(everyone, 128)
    step, new_weights, copied_k, copied_v = call(
        weight_kernel,
        [
            jax.ShapeDtypeStruct(weights.shape, f32),
            jax.ShapeDtypeStruct(weights.shape, f32),
            pltpu.VMEM((RING, rows, columns), bf16),
            pltpu.VMEM((RING, rows, columns), bf16),
        ],
        [VMEM] * 9,
        10,
    )(sums, *keys, *values)
    copied_v = [copied_v, *exchange(copied_v, X)]
    copied_k = [copied_k, *exchange(copied_k, Z)]

    new_left, new_right = call(
        functools.partial(stat_kernel, rows),
        [
            jax.ShapeDtypeStruct((2, rows, features), f32),
            jax.ShapeDtypeStruct((2, columns, columns), f32),
        ],
        [VMEM] * 6,
        20,
    )(left_stat[:, 0], right_stat[:, 0], line_k, line_v, halves_k, halves_v)

    def placed(chosen, *before):
        return call(
            functools.partial(place_kernel, rows, chosen),
            jax.ShapeDtypeStruct((2, features, columns), bf16),
            [VMEM] * len(chosen) + [HBM] * len(before),
            4,
            [pltpu.SemaphoreType.DMA((RING * len(chosen),))],
            out_specs=HBM,
            aliases={len(chosen): 0} if before else None,
        )(*[(copied_k, copied_v)[m][p] for m, p in chosen], *before)

    copies = placed([(1, 0), (0, 0), (1, 1), (0, 1)])
    copies = placed([(1, 2), (0, 2)], copies)
    copies = placed([(1, 3), (0, 3)], copies)
    return (step, new_weights, copies, new_left[:, None], new_right[:, None])


def solution(mesh):
    rings = Mesh(mesh.devices.reshape(4, 4, 4, 2), ("fs_0", "fs_1", "tp_0", "tp_1"))
    in_specs = (
        P(FS, None),
        P(FS, TP),
        P(FS, TP),
        P(None, FS, TP),
        P(None, TP, FS, None),
        P(None, TP, FS, None),
        P(None, TP, None, None),
        P(None, TP, None, None),
    )
    out_specs = (
        P(None, FS, TP),
        P(None, FS, TP),
        P(None, None, TP),
        P(None, TP, FS, None),
        P(None, TP, None, None),
    )

    return jax.shard_map(on_device, mesh=rings, in_specs=in_specs, out_specs=out_specs, check_vma=False)
```

```python
import functools
import math

import jax
import jax.numpy as jnp
from jax import lax
from jax.experimental import pallas as pl
from jax.experimental.pallas import tpu as pltpu
from jax.sharding import Mesh
from jax.sharding import PartitionSpec as P


FS = ("fs_0", "fs_1")
FS_TP = ("fs_0", "fs_1", "tp_0", "tp_1")
TP = ("tp_0", "tp_1")
Z, X = FS
RING = 4
GROUPS = 8
SPAN = 250.0
FLOOR = 124.0
LN2 = math.log(2.0)
MIB = 1 << 20

decay_stat = 0.9
learn_rate = 0.05
norm_eps = 1e-06


VMEM = pl.BlockSpec(memory_space=pltpu.VMEM)
HBM = pl.BlockSpec(memory_space=pl.ANY)


def call(kernel, out_shape, in_specs, limit, scratch=(), out_specs=None, aliases=None):
    single = not isinstance(out_shape, (list, tuple))
    if out_specs is None:
        out_specs = VMEM if single else [VMEM] * len(out_shape)
    return pl.pallas_call(
        kernel,
        out_shape=out_shape,
        in_specs=in_specs,
        out_specs=out_specs,
        scratch_shapes=list(scratch),
        input_output_aliases=aliases or {},
        compiler_params=pltpu.CompilerParams(vmem_limit_bytes=limit * MIB),
    )


def shift(value, axis, by):
    return lax.ppermute(value, axis, [(i, (i + by) % RING) for i in range(RING)])


def where_am_i():
    return lax.axis_index(Z), lax.axis_index(X)


def turn(index):
    return lax.rem(index, RING)


def lanes(index, width):
    return pl.ds(pl.multiple_of(index * width, width), width)


def encode(block, ref, j):
    columns, width = block.shape
    grouped = block.reshape(columns // GROUPS, GROUPS, width)
    size = jnp.abs(grouped)
    scale = (jnp.max(size, axis=0) * 1.0079 + 1e-30).astype(jnp.bfloat16)
    factor = SPAN / scale.astype(jnp.float32)
    code = jnp.exp2(size * factor[None] - FLOOR)
    code = jnp.where(grouped < 0.0, -code, code)
    ref[j, :columns, :] = code.reshape(columns, width).astype(jnp.bfloat16)
    ref[j, columns:, :] = scale


def decode(ref, j):
    rows, width = ref.shape[1:]
    columns = rows - GROUPS
    code = ref[j, :columns, :].astype(jnp.float32).reshape(columns // GROUPS, GROUPS, width)
    scale = ref[j, columns:, :].astype(jnp.float32) * (1.0 / (SPAN * LN2))
    size = (jnp.log(jnp.abs(code)) + FLOOR * LN2) * scale[None]
    return jnp.where(code < 0.0, -size, size).reshape(columns, width)


def split(value):
    high = value.astype(jnp.bfloat16)
    return high, (value - high.astype(jnp.float32)).astype(jnp.bfloat16)


def dot3(left, right, dims):
    (lh, ll), (rh, rl) = left, right
    dot = functools.partial(
        lax.dot_general, dimension_numbers=(dims, ((), ())), preferred_element_type=jnp.float32
    )
    return dot(lh, rh) + (dot(lh, rl) + dot(ll, rh))


def chunk(turned, x_ref, width, m, by):
    z, x = where_am_i()
    if m == 0:
        at = turn(x + by)
        columns = [x_ref[:, lanes(j * RING + at, width)] for j in range(RING)]
        columns = jnp.concatenate(columns, axis=1)
    else:
        columns = x_ref[:, lanes(turn(z + by), RING * width)]
    return jnp.dot(turned, columns, preferred_element_type=jnp.float32)


def coded_chunk(turned, x_ref, width, m, by, out):
    total = chunk(turned, x_ref, width, m, by)
    for j in range(RING):
        encode(total[:, j * width : (j + 1) * width], out, j)


def columns_of(x_hbm, x_ref, width, down, by):
    z, x = where_am_i()
    at = lanes(turn(z + down) * RING + turn(x + by), width)
    return x_hbm.at[:, at], x_ref.at[:, at]


def started(parts, sems):
    copies = [pltpu.make_async_copy(a, b, sems.at[i]) for i, (a, b) in enumerate(parts)]
    for c in copies:
        c.start()
    return copies


def first_kernel(width, x_hbm, k_hbm, v_hbm, x_ref, kt_ref, vt_ref, out_k, out_v, k_ref, v_ref, sems):
    z, _ = where_am_i()
    at = lanes(turn(z + 2), RING * width)
    parts = [(v_hbm, v_ref), (k_hbm, k_ref), (x_hbm.at[:, at], x_ref.at[:, at])]
    for by in (2, 1, 3, 0):
        parts += [columns_of(x_hbm, x_ref, width, down, by) for down in (1, 3, 0)]
    copies = started(parts, sems)
    copies[0].wait()
    vt_ref[...] = v_ref[...].T
    copies[1].wait()
    kt_ref[...] = k_ref[...].T
    copies[2].wait()
    coded_chunk(vt_ref[...], x_ref, width, 1, 2, out_v)
    for c in copies[3:6]:
        c.wait()
    coded_chunk(kt_ref[...], x_ref, width, 0, 2, out_k)
    for c in copies[6:]:
        c.wait()


def near_kernel(width, x_ref, kt_ref, vt_ref, *outs):
    for i, (m, by) in enumerate(((1, 1), (0, 1), (1, 3), (0, 3))):
        coded_chunk((kt_ref, vt_ref)[m][...], x_ref, width, m, by, outs[i])


def own_kernel(width, x_ref, kt_ref, vt_ref, *outs):
    for m in range(2):
        total = chunk((kt_ref, vt_ref)[m][...], x_ref, width, m, 0)
        for j in range(RING):
            outs[m][j] = total[:, j * width : (j + 1) * width]


def sum_kernel(own_ref, a_ref, b_ref, c_ref, total_ref, *codes):
    for j in range(RING):
        total = (own_ref[j] + decode(a_ref, j)) + (decode(b_ref, j) + decode(c_ref, j))
        total_ref[j] = total
        encode(total, codes[j // 2], j % 2)


def pair_kernel(own_ref, a_ref, b_ref, total_ref, *codes):
    for j in range(RING):
        total = own_ref[j] + decode((a_ref, b_ref)[j // 2], j % 2)
        total_ref[j] = total
        if len(codes) == 1:
            encode(total, codes[0], j)
        else:
            encode(total, codes[j // 2], j % 2)


def swap(value, axis, kind):
    return lax.ppermute(value, axis, [(i, i ^ 1 if kind == 0 else 3 - i) for i in range(RING)])


def exchange(blocks, axis):
    return [shift(blocks, axis, s) for s in (2, 1, 3)]


OFFSETS = (2, 3, 1)


def row_block(m, offset, j):
    z, x = where_am_i()
    if m == 0:
        return j * RING + turn(x + offset)
    return turn(z + offset) * RING + j


def raw_kernel(width, m, left_ref, right_ref, before_ref, weights_ref, line_ref, a_ref, b_ref, c_ref, raw_ref, sums_ref, halves_ref):
    pre = None
    for p, (offset, ref) in enumerate(zip((0, *OFFSETS), (line_ref, a_ref, b_ref, c_ref))):
        for pair in range(2):
            lefts, rights = [], []
            for j in (2 * pair, 2 * pair + 1):
                lefts.append(left_ref[m, :, lanes(row_block(m, offset, j), width)])
                rights.append(ref[j] if p == 0 else decode(ref, j))
            both = split(jnp.concatenate(rights, axis=1))
            halves_ref[p * 2 + pair, 0] = both[0]
            halves_ref[p * 2 + pair, 1] = both[1]
            part = dot3(split(jnp.concatenate(lefts, axis=1)), both, ((1,), (1,)))
            pre = part if pre is None else pre + part
    raw = dot3(split(pre), split(right_ref[m]), ((1,), (0,)))
    raw_ref[0] = raw
    raw_ref[1] = weights_ref[m]
    own = line_ref[where_am_i()[m]]
    lane = lax.broadcasted_iota(jnp.int32, (1, 128), 1)
    mine = jnp.where(lane < 64, jnp.sum(own * own), jnp.sum(raw * raw))
    sums_ref[...] = jnp.where((lane // 32) % 2 == m, mine, before_ref[...])


def weight_kernel(sums_ref, *refs):
    ins, (step_ref, new_ref, *lines) = refs[: 2 * RING], refs[2 * RING :]
    total = jnp.sum(sums_ref[...], axis=0, keepdims=True)
    for m in range(2):
        grad_sq = total[:, m * 32 : m * 32 + 1]
        raw_sq = total[:, 64 + m * 32 : 64 + m * 32 + 1]
        scale = jnp.sqrt(grad_sq / (raw_sq + norm_eps))
        for back in range(RING):
            ref = ins[m * RING + back]
            step = scale * ref[0]
            new = ref[1] - learn_rate * step
            if back == 0:
                step_ref[m] = step
                new_ref[m] = new
            lines[m][back] = new.astype(jnp.bfloat16)


def stat_kernel(width, left_ref, right_ref, line_k, line_v, halves_k, halves_v, new_left_ref, new_right_ref):
    z, x = where_am_i()
    for m in range(2):
        own = split((line_k, line_v)[m][(z, x)[m]])
        gram = None
        for p, offset in enumerate((0, *OFFSETS)):
            for pair in range(2):
                halves = (halves_k, halves_v)[m]
                both = halves[p * 2 + pair, 0], halves[p * 2 + pair, 1]
                part = dot3(both, both, ((1,), (1,)))
                gram = part if gram is None else gram + part
                left = dot3(own, both, ((0,), (0,)))
                for n in range(2):
                    at = lanes(row_block(m, offset, 2 * pair + n), width)
                    new_left_ref[m, :, at] = (
                        decay_stat * left_ref[m, :, at]
                        + (1.0 - decay_stat) * left[:, n * width : (n + 1) * width]
                    )
        new_right_ref[m] = decay_stat * right_ref[m] + (1.0 - decay_stat) * gram


def place_kernel(width, chosen, *refs):
    out_ref, sems = refs[-2:]
    parts = []
    for piece, (m, p) in zip(refs, chosen):
        me, offset = where_am_i()[1 - m], (0, *OFFSETS)[p]
        for back in range(RING):
            at = row_block(1 - m, offset, turn(me + RING - back)) * width
            rows = pl.ds(pl.multiple_of(at, width), width)
            parts.append((piece.at[back], out_ref.at[m, rows, :]))
    for c in started(parts, sems):
        c.wait()


def on_device(
    saved_input, key_cot, value_cot, weights, left_root, left_stat, right_root, right_stat
):
    tokens, features = saved_input.shape
    rows, columns = weights.shape[1:]
    f32, bf16 = jnp.float32, jnp.bfloat16
    blocks = (RING, columns, rows)
    coded = (RING, columns + GROUPS, rows)

    x_hbm, k_hbm, v_hbm = [
        pltpu.with_memory_space_constraint(a, pltpu.HBM) for a in (saved_input, key_cot, value_cot)
    ]
    x_here, kt, vt, k2, v2 = call(
        functools.partial(first_kernel, rows),
        [
            pltpu.VMEM((tokens, features), bf16),
            pltpu.VMEM((columns, tokens), bf16),
            pltpu.VMEM((columns, tokens), bf16),
            pltpu.VMEM(coded, bf16),
            pltpu.VMEM(coded, bf16),
        ],
        [HBM] * 3,
        16,
        [
            pltpu.VMEM((tokens, columns), bf16),
            pltpu.VMEM((tokens, columns), bf16),
            pltpu.SemaphoreType.DMA((15,)),
        ],
    )(x_hbm, k_hbm, v_hbm)
    v2, k2 = shift(v2, Z, 2), shift(k2, X, 2)
    v1, k1, v3, k3 = call(
        functools.partial(near_kernel, rows), [pltpu.VMEM(coded, bf16)] * 4, [VMEM] * 3, 12
    )(x_here, kt, vt)
    v1, k1 = shift(v1, Z, 1), shift(k1, X, 1)
    v3, k3 = shift(v3, Z, 3), shift(k3, X, 3)
    k0, v0 = call(functools.partial(own_kernel, rows), [pltpu.VMEM(blocks, f32)] * 2, [VMEM] * 3, 12)(x_here, kt, vt)

    halves = [pltpu.VMEM((2, columns + GROUPS, rows), bf16)] * 2
    total = pltpu.VMEM(blocks, f32)
    add = call(sum_kernel, [total, *halves], [VMEM] * 4, 16)
    pair = call(pair_kernel, [total, *halves], [VMEM] * 3, 16)
    finish = call(pair_kernel, [total, pltpu.VMEM(coded, bf16)], [VMEM] * 3, 16)

    def swapped(codes, axis, step):
        return [swap(c, axis, (h + step) % 2) for h, c in enumerate(codes)]

    v0, *codes_v = add(v0, v2, v1, v3)
    got_v = swapped(codes_v, X, 0)
    k0, *codes_k = add(k0, k2, k1, k3)
    got_k = swapped(codes_k, Z, 0)
    v0, *codes_v = pair(v0, *got_v)
    got_v = swapped(codes_v, X, 1)
    k0, *codes_k = pair(k0, *got_k)
    got_k = swapped(codes_k, Z, 1)
    line_v, code_v = finish(v0, *got_v)
    pieces_v = exchange(code_v, Z)
    line_k, code_k = finish(k0, *got_k)
    pieces_k = exchange(code_k, X)

    def direction(m, before, line, pieces):
        return call(
            functools.partial(raw_kernel, rows, m),
            [
                pltpu.VMEM((2, rows, columns), f32),
                pltpu.VMEM((1, 128), f32),
                pltpu.VMEM((2 * RING, 2, columns, 2 * rows), bf16),
            ],
            [VMEM] * 8,
            12,
        )(left_root[:, 0], right_root[:, 0], before, weights, line, *pieces)

    value, sums, halves_v = direction(1, jnp.zeros((1, 128), f32), line_v, pieces_v)
    values = [value, *[shift(value, Z, s) for s in (1, 2, 3)]]
    key, sums, halves_k = direction(0, sums, line_k, pieces_k)
    keys = [key, *[shift(key, X, s) for s in (1, 2, 3)]]

    everyone = lax.axis_size(FS_TP)
    spread = jnp.broadcast_to(sums[None], (everyone, 1, 128))
    sums = lax.all_to_all(spread, FS_TP, 0, 0, tiled=True).reshape(everyone, 128)
    step, new_weights, copied_k, copied_v = call(
        weight_kernel,
        [
            jax.ShapeDtypeStruct(weights.shape, f32),
            jax.ShapeDtypeStruct(weights.shape, f32),
            pltpu.VMEM((RING, rows, columns), bf16),
            pltpu.VMEM((RING, rows, columns), bf16),
        ],
        [VMEM] * 9,
        10,
    )(sums, *keys, *values)
    copied_v = [copied_v, *exchange(copied_v, X)]
    copied_k = [copied_k, *exchange(copied_k, Z)]

    new_left, new_right = call(
        functools.partial(stat_kernel, rows),
        [
            jax.ShapeDtypeStruct((2, rows, features), f32),
            jax.ShapeDtypeStruct((2, columns, columns), f32),
        ],
        [VMEM] * 6,
        20,
    )(left_stat[:, 0], right_stat[:, 0], line_k, line_v, halves_k, halves_v)

    def placed(chosen, *before):
        return call(
            functools.partial(place_kernel, rows, chosen),
            jax.ShapeDtypeStruct((2, features, columns), bf16),
            [VMEM] * len(chosen) + [HBM] * len(before),
            4,
            [pltpu.SemaphoreType.DMA((RING * len(chosen),))],
            out_specs=HBM,
            aliases={len(chosen): 0} if before else None,
        )(*[(copied_k, copied_v)[m][p] for m, p in chosen], *before)

    copies = placed([(1, 0), (0, 0), (1, 1), (0, 1)])
    copies = placed([(1, 2), (0, 2)], copies)
    copies = placed([(1, 3), (0, 3)], copies)
    return (step, new_weights, copies, new_left[:, None], new_right[:, None])


def solution(mesh):
    rings = Mesh(mesh.devices.reshape(4, 4, 4, 2), ("fs_0", "fs_1", "tp_0", "tp_1"))
    in_specs = (
        P(FS, None),
        P(FS, TP),
        P(FS, TP),
        P(None, FS, TP),
        P(None, TP, FS, None),
        P(None, TP, FS, None),
        P(None, TP, None, None),
        P(None, TP, None, None),
    )
    out_specs = (
        P(None, FS, TP),
        P(None, FS, TP),
        P(None, None, TP),
        P(None, TP, FS, None),
        P(None, TP, None, None),
    )

    return jax.shard_map(on_device, mesh=rings, in_specs=in_specs, out_specs=out_specs, check_vma=False)
```

```python
import functools
import math

import jax
import jax.numpy as jnp
from jax import lax
from jax.experimental import pallas as pl
from jax.experimental.pallas import tpu as pltpu
from jax.sharding import Mesh
from jax.sharding import PartitionSpec as P


FS = ("fs_0", "fs_1")
FS_TP = ("fs_0", "fs_1", "tp_0", "tp_1")
TP = ("tp_0", "tp_1")
Z, X = FS
RING = 4
GROUPS = 8
SPAN = 250.0
FLOOR = 124.0
LN2 = math.log(2.0)
MIB = 1 << 20

decay_stat = 0.9
learn_rate = 0.05
norm_eps = 1e-06


VMEM = pl.BlockSpec(memory_space=pltpu.VMEM)
HBM = pl.BlockSpec(memory_space=pl.ANY)


def call(kernel, out_shape, in_specs, limit, scratch=(), out_specs=None, aliases=None):
    single = not isinstance(out_shape, (list, tuple))
    if out_specs is None:
        out_specs = VMEM if single else [VMEM] * len(out_shape)
    return pl.pallas_call(
        kernel,
        out_shape=out_shape,
        in_specs=in_specs,
        out_specs=out_specs,
        scratch_shapes=list(scratch),
        input_output_aliases=aliases or {},
        compiler_params=pltpu.CompilerParams(vmem_limit_bytes=limit * MIB),
    )


def shift(value, axis, by):
    return lax.ppermute(value, axis, [(i, (i + by) % RING) for i in range(RING)])


def where_am_i():
    return lax.axis_index(Z), lax.axis_index(X)


def turn(index):
    return lax.rem(index, RING)


def lanes(index, width):
    return pl.ds(pl.multiple_of(index * width, width), width)


def encode(block, ref, j):
    columns, width = block.shape
    grouped = block.reshape(columns // GROUPS, GROUPS, width)
    size = jnp.abs(grouped)
    scale = (jnp.max(size, axis=0) * 1.0079 + 1e-30).astype(jnp.bfloat16)
    factor = SPAN / scale.astype(jnp.float32)
    code = jnp.exp2(size * factor[None] - FLOOR)
    code = jnp.where(grouped < 0.0, -code, code)
    ref[j, :columns, :] = code.reshape(columns, width).astype(jnp.bfloat16)
    ref[j, columns:, :] = scale


def decode(ref, j):
    rows, width = ref.shape[1:]
    columns = rows - GROUPS
    code = ref[j, :columns, :].astype(jnp.float32).reshape(columns // GROUPS, GROUPS, width)
    scale = ref[j, columns:, :].astype(jnp.float32) * (1.0 / (SPAN * LN2))
    size = (jnp.log(jnp.abs(code)) + FLOOR * LN2) * scale[None]
    return jnp.where(code < 0.0, -size, size).reshape(columns, width)


def split(value):
    high = value.astype(jnp.bfloat16)
    return high, (value - high.astype(jnp.float32)).astype(jnp.bfloat16)


def dot3(left, right, dims):
    (lh, ll), (rh, rl) = left, right
    dot = functools.partial(
        lax.dot_general, dimension_numbers=(dims, ((), ())), preferred_element_type=jnp.float32
    )
    return dot(lh, rh) + (dot(lh, rl) + dot(ll, rh))


def chunk(turned, x_ref, width, m, by):
    z, x = where_am_i()
    if m == 0:
        at = turn(x + by)
        columns = [x_ref[:, lanes(j * RING + at, width)] for j in range(RING)]
        columns = jnp.concatenate(columns, axis=1)
    else:
        columns = x_ref[:, lanes(turn(z + by), RING * width)]
    return jnp.dot(turned, columns, preferred_element_type=jnp.float32)


def coded_chunk(turned, x_ref, width, m, by, out):
    total = chunk(turned, x_ref, width, m, by)
    for j in range(RING):
        encode(total[:, j * width : (j + 1) * width], out, j)


def columns_of(x_hbm, x_ref, width, down, by):
    z, x = where_am_i()
    at = lanes(turn(z + down) * RING + turn(x + by), width)
    return x_hbm.at[:, at], x_ref.at[:, at]


def started(parts, sems):
    copies = [pltpu.make_async_copy(a, b, sems.at[i]) for i, (a, b) in enumerate(parts)]
    for c in copies:
        c.start()
    return copies


def first_kernel(width, x_hbm, k_hbm, v_hbm, x_ref, kt_ref, vt_ref, out_k, out_v, k_ref, v_ref, sems):
    z, _ = where_am_i()
    at = lanes(turn(z + 2), RING * width)
    parts = [(v_hbm, v_ref), (k_hbm, k_ref), (x_hbm.at[:, at], x_ref.at[:, at])]
    for by in (2, 1, 3, 0):
        parts += [columns_of(x_hbm, x_ref, width, down, by) for down in (1, 3, 0)]
    copies = started(parts, sems)
    copies[0].wait()
    vt_ref[...] = v_ref[...].T
    copies[1].wait()
    kt_ref[...] = k_ref[...].T
    copies[2].wait()
    coded_chunk(vt_ref[...], x_ref, width, 1, 2, out_v)
    for c in copies[3:6]:
        c.wait()
    coded_chunk(kt_ref[...], x_ref, width, 0, 2, out_k)
    for c in copies[6:]:
        c.wait()


def near_kernel(width, x_ref, kt_ref, vt_ref, *outs):
    for i, (m, by) in enumerate(((1, 1), (0, 1), (1, 3), (0, 3))):
        coded_chunk((kt_ref, vt_ref)[m][...], x_ref, width, m, by, outs[i])


def own_kernel(width, x_ref, kt_ref, vt_ref, *outs):
    for m in range(2):
        total = chunk((kt_ref, vt_ref)[m][...], x_ref, width, m, 0)
        for j in range(RING):
            outs[m][j] = total[:, j * width : (j + 1) * width]


def sum_kernel(own_ref, a_ref, b_ref, c_ref, total_ref, *codes):
    for j in range(RING):
        total = (own_ref[j] + decode(a_ref, j)) + (decode(b_ref, j) + decode(c_ref, j))
        total_ref[j] = total
        encode(total, codes[j // 2], j % 2)


def pair_kernel(own_ref, a_ref, b_ref, total_ref, *codes):
    for j in range(RING):
        total = own_ref[j] + decode((a_ref, b_ref)[j // 2], j % 2)
        total_ref[j] = total
        if len(codes) == 1:
            encode(total, codes[0], j)
        else:
            encode(total, codes[j // 2], j % 2)


def swap(value, axis, kind):
    return lax.ppermute(value, axis, [(i, i ^ 1 if kind == 0 else 3 - i) for i in range(RING)])


def exchange(blocks, axis):
    return [shift(blocks, axis, s) for s in (2, 1, 3)]


OFFSETS = (2, 3, 1)


def row_block(m, offset, j):
    z, x = where_am_i()
    if m == 0:
        return j * RING + turn(x + offset)
    return turn(z + offset) * RING + j


def raw_kernel(width, m, left_ref, right_ref, before_ref, weights_ref, line_ref, a_ref, b_ref, c_ref, raw_ref, sums_ref, halves_ref):
    pre = None
    for p, (offset, ref) in enumerate(zip((0, *OFFSETS), (line_ref, a_ref, b_ref, c_ref))):
        for pair in range(2):
            lefts, rights = [], []
            for j in (2 * pair, 2 * pair + 1):
                lefts.append(left_ref[m, :, lanes(row_block(m, offset, j), width)])
                rights.append(ref[j] if p == 0 else decode(ref, j))
            both = split(jnp.concatenate(rights, axis=1))
            halves_ref[p * 2 + pair, 0] = both[0]
            halves_ref[p * 2 + pair, 1] = both[1]
            part = dot3(split(jnp.concatenate(lefts, axis=1)), both, ((1,), (1,)))
            pre = part if pre is None else pre + part
    raw = dot3(split(pre), split(right_ref[m]), ((1,), (0,)))
    raw_ref[0] = raw
    raw_ref[1] = weights_ref[m]
    own = line_ref[where_am_i()[m]]
    lane = lax.broadcasted_iota(jnp.int32, (1, 128), 1)
    mine = jnp.where(lane < 64, jnp.sum(own * own), jnp.sum(raw * raw))
    sums_ref[...] = jnp.where((lane // 32) % 2 == m, mine, before_ref[...])


def weight_kernel(m, sums_ref, *refs):
    ins, (step_ref, new_ref, line_ref) = refs[:RING], refs[RING:]
    total = jnp.sum(sums_ref[...], axis=0, keepdims=True)
    grad_sq = total[:, m * 32 : m * 32 + 1]
    raw_sq = total[:, 64 + m * 32 : 64 + m * 32 + 1]
    scale = jnp.sqrt(grad_sq / (raw_sq + norm_eps))
    for back in range(RING):
        step = scale * ins[back][0]
        new = ins[back][1] - learn_rate * step
        if back == 0:
            step_ref[...] = step
            new_ref[...] = new
        line_ref[back] = new.astype(jnp.bfloat16)


def stat_kernel(width, left_ref, right_ref, line_k, line_v, halves_k, halves_v, new_left_ref, new_right_ref):
    z, x = where_am_i()
    for m in range(2):
        own = split((line_k, line_v)[m][(z, x)[m]])
        gram = None
        for p, offset in enumerate((0, *OFFSETS)):
            for pair in range(2):
                halves = (halves_k, halves_v)[m]
                both = halves[p * 2 + pair, 0], halves[p * 2 + pair, 1]
                part = dot3(both, both, ((1,), (1,)))
                gram = part if gram is None else gram + part
                left = dot3(own, both, ((0,), (0,)))
                for n in range(2):
                    at = lanes(row_block(m, offset, 2 * pair + n), width)
                    new_left_ref[m, :, at] = (
                        decay_stat * left_ref[m, :, at]
                        + (1.0 - decay_stat) * left[:, n * width : (n + 1) * width]
                    )
        new_right_ref[m] = decay_stat * right_ref[m] + (1.0 - decay_stat) * gram


def place_kernel(width, chosen, *refs):
    out_ref, sems = refs[-2:]
    parts = []
    for piece, (m, p) in zip(refs, chosen):
        me, offset = where_am_i()[1 - m], (0, *OFFSETS)[p]
        for back in range(RING):
            at = row_block(1 - m, offset, turn(me + RING - back)) * width
            rows = pl.ds(pl.multiple_of(at, width), width)
            parts.append((piece.at[back], out_ref.at[m, rows, :]))
    for c in started(parts, sems):
        c.wait()


def on_device(
    saved_input, key_cot, value_cot, weights, left_root, left_stat, right_root, right_stat
):
    tokens, features = saved_input.shape
    rows, columns = weights.shape[1:]
    f32, bf16 = jnp.float32, jnp.bfloat16
    blocks = (RING, columns, rows)
    coded = (RING, columns + GROUPS, rows)

    x_hbm, k_hbm, v_hbm = [
        pltpu.with_memory_space_constraint(a, pltpu.HBM) for a in (saved_input, key_cot, value_cot)
    ]
    x_here, kt, vt, k2, v2 = call(
        functools.partial(first_kernel, rows),
        [
            pltpu.VMEM((tokens, features), bf16),
            pltpu.VMEM((columns, tokens), bf16),
            pltpu.VMEM((columns, tokens), bf16),
            pltpu.VMEM(coded, bf16),
            pltpu.VMEM(coded, bf16),
        ],
        [HBM] * 3,
        16,
        [
            pltpu.VMEM((tokens, columns), bf16),
            pltpu.VMEM((tokens, columns), bf16),
            pltpu.SemaphoreType.DMA((15,)),
        ],
    )(x_hbm, k_hbm, v_hbm)
    v2, k2 = shift(v2, Z, 2), shift(k2, X, 2)
    v1, k1, v3, k3 = call(
        functools.partial(near_kernel, rows), [pltpu.VMEM(coded, bf16)] * 4, [VMEM] * 3, 12
    )(x_here, kt, vt)
    v1, k1 = shift(v1, Z, 1), shift(k1, X, 1)
    v3, k3 = shift(v3, Z, 3), shift(k3, X, 3)
    k0, v0 = call(functools.partial(own_kernel, rows), [pltpu.VMEM(blocks, f32)] * 2, [VMEM] * 3, 12)(x_here, kt, vt)

    halves = [pltpu.VMEM((2, columns + GROUPS, rows), bf16)] * 2
    total = pltpu.VMEM(blocks, f32)
    add = call(sum_kernel, [total, *halves], [VMEM] * 4, 16)
    pair = call(pair_kernel, [total, *halves], [VMEM] * 3, 16)
    finish = call(pair_kernel, [total, pltpu.VMEM(coded, bf16)], [VMEM] * 3, 16)

    def swapped(codes, axis, step):
        return [swap(c, axis, (h + step) % 2) for h, c in enumerate(codes)]

    v0, *codes_v = add(v0, v2, v1, v3)
    got_v = swapped(codes_v, X, 0)
    k0, *codes_k = add(k0, k2, k1, k3)
    got_k = swapped(codes_k, Z, 0)
    v0, *codes_v = pair(v0, *got_v)
    got_v = swapped(codes_v, X, 1)
    k0, *codes_k = pair(k0, *got_k)
    got_k = swapped(codes_k, Z, 1)
    line_v, code_v = finish(v0, *got_v)
    pieces_v = exchange(code_v, Z)
    line_k, code_k = finish(k0, *got_k)
    pieces_k = exchange(code_k, X)

    def direction(m, before, line, pieces):
        return call(
            functools.partial(raw_kernel, rows, m),
            [
                pltpu.VMEM((2, rows, columns), f32),
                pltpu.VMEM((1, 128), f32),
                pltpu.VMEM((2 * RING, 2, columns, 2 * rows), bf16),
            ],
            [VMEM] * 8,
            12,
        )(left_root[:, 0], right_root[:, 0], before, weights, line, *pieces)

    value, sums, halves_v = direction(1, jnp.zeros((1, 128), f32), line_v, pieces_v)
    values = [value, *[shift(value, Z, s) for s in (1, 2, 3)]]
    key, sums, halves_k = direction(0, sums, line_k, pieces_k)
    keys = [key, *[shift(key, X, s) for s in (1, 2, 3)]]

    everyone = lax.axis_size(FS_TP)
    spread = jnp.broadcast_to(sums[None], (everyone, 1, 128))
    sums = lax.all_to_all(spread, FS_TP, 0, 0, tiled=True).reshape(everyone, 128)

    def updated(m, line):
        one = jax.ShapeDtypeStruct((rows, columns), f32)
        return call(
            functools.partial(weight_kernel, m), [one, one, pltpu.VMEM((RING, rows, columns), bf16)], [VMEM] * 5, 6
        )(sums, *line)

    step_v, new_v, copied_v = updated(1, values)
    step_k, new_k, copied_k = updated(0, keys)
    step, new_weights = jnp.stack([step_k, step_v]), jnp.stack([new_k, new_v])
    copied_v = [copied_v, *exchange(copied_v, X)]
    copied_k = [copied_k, *exchange(copied_k, Z)]

    new_left, new_right = call(
        functools.partial(stat_kernel, rows),
        [
            jax.ShapeDtypeStruct((2, rows, features), f32),
            jax.ShapeDtypeStruct((2, columns, columns), f32),
        ],
        [VMEM] * 6,
        20,
    )(left_stat[:, 0], right_stat[:, 0], line_k, line_v, halves_k, halves_v)

    def placed(chosen, *before):
        return call(
            functools.partial(place_kernel, rows, chosen),
            jax.ShapeDtypeStruct((2, features, columns), bf16),
            [VMEM] * len(chosen) + [HBM] * len(before),
            4,
            [pltpu.SemaphoreType.DMA((RING * len(chosen),))],
            out_specs=HBM,
            aliases={len(chosen): 0} if before else None,
        )(*[(copied_k, copied_v)[m][p] for m, p in chosen], *before)

    copies = placed([(1, 0), (0, 0), (1, 1), (0, 1)])
    copies = placed([(1, 2), (0, 2), (1, 3), (0, 3)], copies)
    return (step, new_weights, copies, new_left[:, None], new_right[:, None])


def solution(mesh):
    rings = Mesh(mesh.devices.reshape(4, 4, 4, 2), ("fs_0", "fs_1", "tp_0", "tp_1"))
    in_specs = (
        P(FS, None),
        P(FS, TP),
        P(FS, TP),
        P(None, FS, TP),
        P(None, TP, FS, None),
        P(None, TP, FS, None),
        P(None, TP, None, None),
        P(None, TP, None, None),
    )
    out_specs = (
        P(None, FS, TP),
        P(None, FS, TP),
        P(None, None, TP),
        P(None, TP, FS, None),
        P(None, TP, None, None),
    )

    return jax.shard_map(on_device, mesh=rings, in_specs=in_specs, out_specs=out_specs, check_vma=False)
```

```python
import functools
import math

import jax
import jax.numpy as jnp
from jax import lax
from jax.experimental import pallas as pl
from jax.experimental.pallas import tpu as pltpu
from jax.sharding import Mesh
from jax.sharding import PartitionSpec as P


FS = ("fs_0", "fs_1")
FS_TP = ("fs_0", "fs_1", "tp_0", "tp_1")
TP = ("tp_0", "tp_1")
Z, X = FS
RING = 4
GROUPS = 8
SPAN = 250.0
FLOOR = 124.0
LN2 = math.log(2.0)
MIB = 1 << 20

decay_stat = 0.9
learn_rate = 0.05
norm_eps = 1e-06


VMEM = pl.BlockSpec(memory_space=pltpu.VMEM)
HBM = pl.BlockSpec(memory_space=pl.ANY)


def call(kernel, out_shape, in_specs, limit, scratch=(), out_specs=None, aliases=None):
    single = not isinstance(out_shape, (list, tuple))
    if out_specs is None:
        out_specs = VMEM if single else [VMEM] * len(out_shape)
    return pl.pallas_call(
        kernel,
        out_shape=out_shape,
        in_specs=in_specs,
        out_specs=out_specs,
        scratch_shapes=list(scratch),
        input_output_aliases=aliases or {},
        compiler_params=pltpu.CompilerParams(vmem_limit_bytes=limit * MIB),
    )


def shift(value, axis, by):
    return lax.ppermute(value, axis, [(i, (i + by) % RING) for i in range(RING)])


def where_am_i():
    return lax.axis_index(Z), lax.axis_index(X)


def turn(index):
    return lax.rem(index, RING)


def lanes(index, width):
    return pl.ds(pl.multiple_of(index * width, width), width)


def encode(block, ref, j):
    columns, width = block.shape
    grouped = block.reshape(columns // GROUPS, GROUPS, width)
    size = jnp.abs(grouped)
    scale = (jnp.max(size, axis=0) * 1.0079 + 1e-30).astype(jnp.bfloat16)
    factor = SPAN / scale.astype(jnp.float32)
    code = jnp.exp2(size * factor[None] - FLOOR)
    code = jnp.where(grouped < 0.0, -code, code)
    ref[j, :columns, :] = code.reshape(columns, width).astype(jnp.bfloat16)
    ref[j, columns:, :] = scale


def decode(ref, j):
    rows, width = ref.shape[1:]
    columns = rows - GROUPS
    code = ref[j, :columns, :].astype(jnp.float32).reshape(columns // GROUPS, GROUPS, width)
    scale = ref[j, columns:, :].astype(jnp.float32) * (1.0 / (SPAN * LN2))
    size = (jnp.log(jnp.abs(code)) + FLOOR * LN2) * scale[None]
    return jnp.where(code < 0.0, -size, size).reshape(columns, width)


def split(value):
    high = value.astype(jnp.bfloat16)
    return high, (value - high.astype(jnp.float32)).astype(jnp.bfloat16)


def dot3(left, right, dims):
    (lh, ll), (rh, rl) = left, right
    free = 1 - dims[0][0]
    dot = functools.partial(
        lax.dot_general, dimension_numbers=(dims, ((), ())), preferred_element_type=jnp.float32
    )
    both = dot(jnp.concatenate([lh, ll], axis=free), rh)
    count = lh.shape[free]
    return both[:count] + (dot(lh, rl) + both[count:])


def chunk(turned, x_ref, width, m, by):
    z, x = where_am_i()
    if m == 0:
        at = turn(x + by)
        columns = [x_ref[:, lanes(j * RING + at, width)] for j in range(RING)]
        columns = jnp.concatenate(columns, axis=1)
    else:
        columns = x_ref[:, lanes(turn(z + by), RING * width)]
    return jnp.dot(turned, columns, preferred_element_type=jnp.float32)


def coded_chunk(turned, x_ref, width, m, by, out):
    total = chunk(turned, x_ref, width, m, by)
    for j in range(RING):
        encode(total[:, j * width : (j + 1) * width], out, j)


def columns_of(x_hbm, x_ref, width, down, by):
    z, x = where_am_i()
    at = lanes(turn(z + down) * RING + turn(x + by), width)
    return x_hbm.at[:, at], x_ref.at[:, at]


def started(parts, sems):
    copies = [pltpu.make_async_copy(a, b, sems.at[i]) for i, (a, b) in enumerate(parts)]
    for c in copies:
        c.start()
    return copies


def first_kernel(width, x_hbm, k_hbm, v_hbm, x_ref, kt_ref, vt_ref, out_k, out_v, k_ref, v_ref, sems):
    z, _ = where_am_i()
    at = lanes(turn(z + 2), RING * width)
    parts = [(v_hbm, v_ref), (k_hbm, k_ref), (x_hbm.at[:, at], x_ref.at[:, at])]
    for by in (2, 1, 3, 0):
        parts += [columns_of(x_hbm, x_ref, width, down, by) for down in (1, 3, 0)]
    copies = started(parts, sems)
    copies[0].wait()
    vt_ref[...] = v_ref[...].T
    copies[1].wait()
    kt_ref[...] = k_ref[...].T
    copies[2].wait()
    coded_chunk(vt_ref[...], x_ref, width, 1, 2, out_v)
    for c in copies[3:6]:
        c.wait()
    coded_chunk(kt_ref[...], x_ref, width, 0, 2, out_k)
    for c in copies[6:]:
        c.wait()


def near_kernel(width, x_ref, kt_ref, vt_ref, *outs):
    for i, (m, by) in enumerate(((1, 1), (0, 1), (1, 3), (0, 3))):
        coded_chunk((kt_ref, vt_ref)[m][...], x_ref, width, m, by, outs[i])


def own_kernel(width, x_ref, kt_ref, vt_ref, *outs):
    for m in range(2):
        total = chunk((kt_ref, vt_ref)[m][...], x_ref, width, m, 0)
        for j in range(RING):
            outs[m][j] = total[:, j * width : (j + 1) * width]


def sum_kernel(own_ref, a_ref, b_ref, c_ref, total_ref, *codes):
    for j in range(RING):
        total = (own_ref[j] + decode(a_ref, j)) + (decode(b_ref, j) + decode(c_ref, j))
        total_ref[j] = total
        encode(total, codes[j // 2], j % 2)


def pair_kernel(own_ref, a_ref, b_ref, total_ref, *codes):
    for j in range(RING):
        total = own_ref[j] + decode((a_ref, b_ref)[j // 2], j % 2)
        total_ref[j] = total
        if len(codes) == 1:
            encode(total, codes[0], j)
        else:
            encode(total, codes[j // 2], j % 2)


def swap(value, axis, kind):
    return lax.ppermute(value, axis, [(i, i ^ 1 if kind == 0 else 3 - i) for i in range(RING)])


def exchange(blocks, axis):
    return [shift(blocks, axis, s) for s in (2, 1, 3)]


OFFSETS = (2, 3, 1)


def row_block(m, offset, j):
    z, x = where_am_i()
    if m == 0:
        return j * RING + turn(x + offset)
    return turn(z + offset) * RING + j


def raw_kernel(width, m, left_ref, right_ref, before_ref, weights_ref, line_ref, a_ref, b_ref, c_ref, raw_ref, sums_ref, halves_ref):
    pre = None
    for p, (offset, ref) in enumerate(zip((0, *OFFSETS), (line_ref, a_ref, b_ref, c_ref))):
        for pair in range(2):
            lefts, rights = [], []
            for j in (2 * pair, 2 * pair + 1):
                lefts.append(left_ref[m, :, lanes(row_block(m, offset, j), width)])
                rights.append(ref[j] if p == 0 else decode(ref, j))
            both = split(jnp.concatenate(rights, axis=1))
            halves_ref[p * 2 + pair, 0] = both[0]
            halves_ref[p * 2 + pair, 1] = both[1]
            part = dot3(split(jnp.concatenate(lefts, axis=1)), both, ((1,), (1,)))
            pre = part if pre is None else pre + part
    raw = dot3(split(pre), split(right_ref[m]), ((1,), (0,)))
    raw_ref[0] = raw
    raw_ref[1] = weights_ref[m]
    own = line_ref[where_am_i()[m]]
    lane = lax.broadcasted_iota(jnp.int32, (1, 128), 1)
    mine = jnp.where(lane < 64, jnp.sum(own * own), jnp.sum(raw * raw))
    sums_ref[...] = jnp.where((lane // 32) % 2 == m, mine, before_ref[...])


def weight_kernel(m, sums_ref, *refs):
    ins, (step_ref, new_ref, line_ref) = refs[:RING], refs[RING:]
    total = jnp.sum(sums_ref[...], axis=0, keepdims=True)
    grad_sq = total[:, m * 32 : m * 32 + 1]
    raw_sq = total[:, 64 + m * 32 : 64 + m * 32 + 1]
    scale = jnp.sqrt(grad_sq / (raw_sq + norm_eps))
    for back in range(RING):
        step = scale * ins[back][0]
        new = ins[back][1] - learn_rate * step
        if back == 0:
            step_ref[...] = step
            new_ref[...] = new
        line_ref[back] = new.astype(jnp.bfloat16)


def stat_kernel(width, left_ref, right_ref, line_k, line_v, halves_k, halves_v, new_left_ref, new_right_ref):
    z, x = where_am_i()
    for m in range(2):
        own = split((line_k, line_v)[m][(z, x)[m]])
        gram = None
        for p, offset in enumerate((0, *OFFSETS)):
            for pair in range(2):
                halves = (halves_k, halves_v)[m]
                both = halves[p * 2 + pair, 0], halves[p * 2 + pair, 1]
                part = dot3(both, both, ((1,), (1,)))
                gram = part if gram is None else gram + part
                left = dot3(own, both, ((0,), (0,)))
                for n in range(2):
                    at = lanes(row_block(m, offset, 2 * pair + n), width)
                    new_left_ref[m, :, at] = (
                        decay_stat * left_ref[m, :, at]
                        + (1.0 - decay_stat) * left[:, n * width : (n + 1) * width]
                    )
        new_right_ref[m] = decay_stat * right_ref[m] + (1.0 - decay_stat) * gram


def place_kernel(width, chosen, *refs):
    out_ref, sems = refs[-2:]
    parts = []
    for piece, (m, p) in zip(refs, chosen):
        me, offset = where_am_i()[1 - m], (0, *OFFSETS)[p]
        for back in range(RING):
            at = row_block(1 - m, offset, turn(me + RING - back)) * width
            rows = pl.ds(pl.multiple_of(at, width), width)
            parts.append((piece.at[back], out_ref.at[m, rows, :]))
    for c in started(parts, sems):
        c.wait()


def on_device(
    saved_input, key_cot, value_cot, weights, left_root, left_stat, right_root, right_stat
):
    tokens, features = saved_input.shape
    rows, columns = weights.shape[1:]
    f32, bf16 = jnp.float32, jnp.bfloat16
    blocks = (RING, columns, rows)
    coded = (RING, columns + GROUPS, rows)

    x_hbm, k_hbm, v_hbm = [
        pltpu.with_memory_space_constraint(a, pltpu.HBM) for a in (saved_input, key_cot, value_cot)
    ]
    x_here, kt, vt, k2, v2 = call(
        functools.partial(first_kernel, rows),
        [
            pltpu.VMEM((tokens, features), bf16),
            pltpu.VMEM((columns, tokens), bf16),
            pltpu.VMEM((columns, tokens), bf16),
            pltpu.VMEM(coded, bf16),
            pltpu.VMEM(coded, bf16),
        ],
        [HBM] * 3,
        16,
        [
            pltpu.VMEM((tokens, columns), bf16),
            pltpu.VMEM((tokens, columns), bf16),
            pltpu.SemaphoreType.DMA((15,)),
        ],
    )(x_hbm, k_hbm, v_hbm)
    v2, k2 = shift(v2, Z, 2), shift(k2, X, 2)
    v1, k1, v3, k3 = call(
        functools.partial(near_kernel, rows), [pltpu.VMEM(coded, bf16)] * 4, [VMEM] * 3, 12
    )(x_here, kt, vt)
    v1, k1 = shift(v1, Z, 1), shift(k1, X, 1)
    v3, k3 = shift(v3, Z, 3), shift(k3, X, 3)
    k0, v0 = call(functools.partial(own_kernel, rows), [pltpu.VMEM(blocks, f32)] * 2, [VMEM] * 3, 12)(x_here, kt, vt)

    halves = [pltpu.VMEM((2, columns + GROUPS, rows), bf16)] * 2
    total = pltpu.VMEM(blocks, f32)
    add = call(sum_kernel, [total, *halves], [VMEM] * 4, 16)
    pair = call(pair_kernel, [total, *halves], [VMEM] * 3, 16)
    finish = call(pair_kernel, [total, pltpu.VMEM(coded, bf16)], [VMEM] * 3, 16)

    def swapped(codes, axis, step):
        return [swap(c, axis, (h + step) % 2) for h, c in enumerate(codes)]

    v0, *codes_v = add(v0, v2, v1, v3)
    got_v = swapped(codes_v, X, 0)
    k0, *codes_k = add(k0, k2, k1, k3)
    got_k = swapped(codes_k, Z, 0)
    v0, *codes_v = pair(v0, *got_v)
    got_v = swapped(codes_v, X, 1)
    k0, *codes_k = pair(k0, *got_k)
    got_k = swapped(codes_k, Z, 1)
    line_v, code_v = finish(v0, *got_v)
    pieces_v = exchange(code_v, Z)
    line_k, code_k = finish(k0, *got_k)
    pieces_k = exchange(code_k, X)

    def direction(m, before, line, pieces):
        return call(
            functools.partial(raw_kernel, rows, m),
            [
                pltpu.VMEM((2, rows, columns), f32),
                pltpu.VMEM((1, 128), f32),
                pltpu.VMEM((2 * RING, 2, columns, 2 * rows), bf16),
            ],
            [VMEM] * 8,
            12,
        )(left_root[:, 0], right_root[:, 0], before, weights, line, *pieces)

    value, sums, halves_v = direction(1, jnp.zeros((1, 128), f32), line_v, pieces_v)
    values = [value, *[shift(value, Z, s) for s in (1, 2, 3)]]
    key, sums, halves_k = direction(0, sums, line_k, pieces_k)
    keys = [key, *[shift(key, X, s) for s in (1, 2, 3)]]

    everyone = lax.axis_size(FS_TP)
    spread = jnp.broadcast_to(sums[None], (everyone, 1, 128))
    sums = lax.all_to_all(spread, FS_TP, 0, 0, tiled=True).reshape(everyone, 128)

    def updated(m, line):
        one = jax.ShapeDtypeStruct((rows, columns), f32)
        return call(
            functools.partial(weight_kernel, m), [one, one, pltpu.VMEM((RING, rows, columns), bf16)], [VMEM] * 5, 6
        )(sums, *line)

    step_v, new_v, copied_v = updated(1, values)
    step_k, new_k, copied_k = updated(0, keys)
    step, new_weights = jnp.stack([step_k, step_v]), jnp.stack([new_k, new_v])
    copied_v = [copied_v, *exchange(copied_v, X)]
    copied_k = [copied_k, *exchange(copied_k, Z)]

    new_left, new_right = call(
        functools.partial(stat_kernel, rows),
        [
            jax.ShapeDtypeStruct((2, rows, features), f32),
            jax.ShapeDtypeStruct((2, columns, columns), f32),
        ],
        [VMEM] * 6,
        20,
    )(left_stat[:, 0], right_stat[:, 0], line_k, line_v, halves_k, halves_v)

    def placed(chosen, *before):
        return call(
            functools.partial(place_kernel, rows, chosen),
            jax.ShapeDtypeStruct((2, features, columns), bf16),
            [VMEM] * len(chosen) + [HBM] * len(before),
            4,
            [pltpu.SemaphoreType.DMA((RING * len(chosen),))],
            out_specs=HBM,
            aliases={len(chosen): 0} if before else None,
        )(*[(copied_k, copied_v)[m][p] for m, p in chosen], *before)

    copies = placed([(1, 0), (0, 0), (1, 1), (0, 1)])
    copies = placed([(1, 2), (0, 2), (1, 3), (0, 3)], copies)
    return (step, new_weights, copies, new_left[:, None], new_right[:, None])


def solution(mesh):
    rings = Mesh(mesh.devices.reshape(4, 4, 4, 2), ("fs_0", "fs_1", "tp_0", "tp_1"))
    in_specs = (
        P(FS, None),
        P(FS, TP),
        P(FS, TP),
        P(None, FS, TP),
        P(None, TP, FS, None),
        P(None, TP, FS, None),
        P(None, TP, None, None),
        P(None, TP, None, None),
    )
    out_specs = (
        P(None, FS, TP),
        P(None, FS, TP),
        P(None, None, TP),
        P(None, TP, FS, None),
        P(None, TP, None, None),
    )

    return jax.shard_map(on_device, mesh=rings, in_specs=in_specs, out_specs=out_specs, check_vma=False)
```
